32 devices in a mesh: ep: 8 (over z, x), tp: 4 (over y, core).
Axes of the slice: x: 2, y: 2, z: 4, core: 2. Of those that a mesh axis runs over, the one named last changes fastest.
Arguments:
- queries: bfloat16 [1024, 512], P('ep'), may hold values from -6 to 6
- key_vectors: bfloat16 [1024, 512], P('ep'), may hold values from -6 to 6
- values: bfloat16 [1024, 1024], P('ep', 'tp'), may hold values from -6 to 6
- out_gate: bfloat16 [1024, 1024], P('ep', 'tp'), may hold values from -6 to 6
- input_gate: float32 [1024, 2], P('ep'), may hold values from -8 to 130
- forget_gate: float32 [1024, 2], P('ep'), may hold values from -2 to 16
- mix_weight: bfloat16 [1024, 2048], P('tp'), may hold values from -0.1875 to 0.1875
- expert_input: bfloat16 [2048, 2048], P('ep'), may hold values from -6 to 6
- norm_gain: float32 [2048], replicated, may hold values from 0.1 to 1.9
- route_ids: int32 [2048, 4], P('ep'), may hold values from 0 to 7, all different within a row; in each aligned block of 256 rows (0 to 255, 256 to 511, ...) at most 256 rows name the same one
- route_weights: float32 [2048, 4], P('ep'), may hold values from 0.2 to 1.2
- expert_gate: bfloat16 [32, 2048, 256], P(('ep', 'tp')), may hold values from -0.125 to 0.125
- expert_up: bfloat16 [32, 2048, 256], P(('ep', 'tp')), may hold values from -0.125 to 0.125
- expert_down: bfloat16 [32, 256, 2048], P(('ep', 'tp')), may hold values from -0.1875 to 0.1875
- shared_gate: bfloat16 [2048, 512], P(None, 'tp'), may hold values from -0.125 to 0.125
- shared_up: bfloat16 [2048, 512], P(None, 'tp'), may hold values from -0.125 to 0.125
- shared_down: bfloat16 [512, 2048], P('tp'), may hold values from -0.25 to 0.25
Outputs:
- mixer_out: bfloat16 [1024, 2048], P('ep')
- expert_out: bfloat16 [2048, 2048], P('ep')
The draws below stay inside these ranges and needn't reach their ends.
Inputs may be any that keep to these rules, and one draw needn't show every extreme that they name: `route_ids`: each row names 4 different experts. In each aligned block of 256 rows (the rows of one index of ep) no expert is named by more than 256 rows, and in some block one expert is named by exactly 256 rows.
All inputs are finite; a program needn't handle non-finite values.
Results may differ from the reference program's by a relative error of at most 0.01575.
Values may be sent and summed in bfloat16 or wider, within the bound.
A program may use at most 64 MiB of HBM per device.

```python
import math
import jax
import jax.numpy as jnp
import numpy as np
from jax import lax

D = 2048
MEMORY_HEADS = 2
KEY_DIM = 256
VAL_DIM = 512
BLOCK = 128
MOE_DEV = 256
TOPK = 4
FF = 1024
FF_SHARED = 512
MIXER_TOKEN_COUNT = 1024
MOE_TOKENS = 2048
TP_GROUP = 4
FF_DEV = 256
EXPERTS = 8
CAP = 256
VAL_DEV = 256
N_EP = 8
N_TP = 4


def draw_input_gate(key, part):
    random_subkeys = jax.random.split(jax.random.fold_in(key, 23), 1)
    pre_gate = jnp.clip(1.5 * jax.random.normal(random_subkeys[0], (MIXER_TOKEN_COUNT, MEMORY_HEADS), jnp.float32), -7.5, 7.5)
    return pre_gate


def draw_forget_gate(key, part):
    random_subkeys = jax.random.split(jax.random.fold_in(key, 41), 5)
    token_positions = jnp.arange(MIXER_TOKEN_COUNT, dtype=jnp.int32)
    shuffled = jax.random.permutation(random_subkeys[0], MEMORY_HEADS)
    slow_heads = (shuffled < MEMORY_HEADS // 2).astype(jnp.float32)
    slow_rate = 0.5
    baseline_rate = slow_heads * (slow_rate / MIXER_TOKEN_COUNT) + (1.0 - slow_heads) / 40.0
    block_multiplier = jnp.exp(jax.random.uniform(random_subkeys[1], (MIXER_TOKEN_COUNT // BLOCK, MEMORY_HEADS), jnp.float32, -0.69, 0.69))
    block_multiplier = jnp.repeat(block_multiplier, BLOCK, axis=0)
    jitter_amount = jnp.exp(jax.random.uniform(random_subkeys[2], (MIXER_TOKEN_COUNT, MEMORY_HEADS), jnp.float32, -1.1, 1.1))
    spike_position = jax.random.randint(random_subkeys[3], (3, MEMORY_HEADS), 0, MIXER_TOKEN_COUNT)
    spike_flag = jnp.any(token_positions[:, None, None] == spike_position[None, :, :], axis=1)
    spike_magnitude = jnp.log(jax.random.uniform(random_subkeys[4], (MIXER_TOKEN_COUNT, MEMORY_HEADS), jnp.float32, 0.5, 0.8))
    log_retention = -baseline_rate[None, :] * block_multiplier * jitter_amount + jnp.where(spike_flag, spike_magnitude, 0.0)
    return log_retention - jnp.log(-jnp.expm1(log_retention))


def levels(stream_key, dims, shards, least, high):
    def one(dim, shards_of):
        steps = jax.random.uniform(jax.random.fold_in(jax.random.fold_in(stream_key, 6), dim), (shards_of,), jnp.float32, least / len(shards), high / len(shards))
        return jnp.repeat(jnp.exp(steps), dims[dim] // shards_of).reshape((-1,) + (1,) * (len(dims) - dim - 1))

    factor_of = one(*shards[0])
    for cut in shards[1:]:
        factor_of = factor_of * one(*cut)
    return factor_of


def deal_out(stream_key, own, number, rows, count, top, limit, lean):
    order = jax.random.permutation(stream_key, count)
    crowded, ordinary = shares(count, rows * top, limit, lean, True), shares(count, rows * top, limit, lean, False)
    places = jnp.arange(count)

    def named(tallies, rotation):
        used = int((tallies > 0).sum())
        fixed = max(1, used // 4)
        shifted = fixed + (places - fixed + rotation * (used - fixed)) % max(1, count - fixed)
        return jnp.zeros((count,), jnp.int32).at[order[jnp.where(places < fixed, places, shifted)]].set(jnp.asarray(tallies, jnp.int32))

    tallies = jnp.where(number % 4 == 0, named(crowded, number // 4), named(ordinary, number - number // 4 - 1))
    mixed = jax.random.permutation(jax.random.fold_in(own, 3), count)
    donor, sink = mixed[0:count // 2 * 2:2], mixed[1:count // 2 * 2:2]
    margin = jnp.minimum(tallies[donor] - 1, limit - tallies[sink]) // 2
    margin = jnp.where((donor == order[0]) | (sink == order[0]) | (tallies[sink] == 0), 0, jnp.maximum(margin, 0))
    shifted = jax.random.randint(jax.random.fold_in(own, 4), (count // 2,), 0, 1 << 20) % (margin + 1)
    tallies = tallies.at[donor].add(-shifted).at[sink].add(shifted)
    members = jnp.searchsorted(jnp.cumsum(tallies), jnp.arange(rows * top), side="right").astype(jnp.int32)
    grid = members.reshape(top, rows).T
    grid = grid[jax.random.permutation(jax.random.fold_in(own, 1), rows)]
    rotation = jax.random.randint(jax.random.fold_in(own, 2), (rows, 1), 0, top)
    return jnp.take_along_axis(grid, (jnp.arange(top)[None, :] + rotation) % top, axis=1)


def shares(count, total, limit, skew, full):
    weights = [(1 << 20) // math.isqrt(standing ** skew) + 1 for standing in range(1, count + 1)]
    largest = limit if full else min(limit, max(-(-total // count), total * weights[0] // sum(weights)))
    least = 1 if total - largest >= count - 1 else 0
    given, rest = [largest] + [least] * (count - 1), total - largest - least * (count - 1)
    while rest > 0:
        free = [i for i in range(1, count) if given[i] < largest] or [i for i in range(1, count) if given[i] < limit]
        pool, left = sum([weights[i] for i in free]), rest
        for i in free:
            extra = min(limit - given[i], max(1, left * weights[i] // pool), rest)
            given[i] = given[i] + extra
            rest = rest - extra
    return np.array(given)


def centred(rng, shape, width, reach, shards=(), held_as=jnp.bfloat16):
    entries = width * jax.random.normal(rng, shape, jnp.float32)
    if shards:
        entries = entries * levels(rng, shape, shards, -0.22, 0.18)
    return jnp.clip(entries, -reach, reach).astype(held_as)


def setup_inputs(seed: int = 0) -> dict:
    keys = jax.random.split(jax.random.key(seed), 18)
    queries = centred(keys[0], (MIXER_TOKEN_COUNT, MEMORY_HEADS * KEY_DIM), 1.0, 6.0, ((0, 8),))
    key_vectors = centred(keys[1], (MIXER_TOKEN_COUNT, MEMORY_HEADS * KEY_DIM), 1.0, 6.0, ((0, 8),))
    values = centred(keys[2], (MIXER_TOKEN_COUNT, MEMORY_HEADS * VAL_DIM), 1.0, 6.0, ((0, 8), (1, 4)))
    out_gate = centred(keys[3], (MIXER_TOKEN_COUNT, MEMORY_HEADS * VAL_DIM), 1.0, 6.0, ((0, 8), (1, 4)))
    input_gate = draw_input_gate(jax.random.fold_in(keys[17], 71), 0)
    forget_gate = draw_forget_gate(jax.random.fold_in(keys[17], 71), 0)
    mix_weight = centred(keys[6], (MEMORY_HEADS * VAL_DIM, D), (MEMORY_HEADS * VAL_DIM) ** -0.5, 0.1875, ((0, 4),))
    expert_input = centred(keys[7], (MOE_TOKENS, D), 1.0, 6.0, ((0, 8),))
    norm_gain = jnp.clip(1.0 + 0.18 * jax.random.normal(keys[8], (D,), jnp.float32), 0.1, 1.9)
    route_ids_keys = jax.random.split(jax.random.fold_in(keys[9], 1), MOE_TOKENS // MOE_DEV)
    route_ids_turns = jax.random.permutation(jax.random.fold_in(keys[9], 3), MOE_TOKENS // MOE_DEV)
    route_ids = jax.vmap(lambda own, number: deal_out(jax.random.fold_in(keys[9], 2), own, number, MOE_DEV, EXPERTS, TOPK, CAP, 2))(route_ids_keys, route_ids_turns).reshape((MOE_TOKENS, TOPK))
    route_weights = jnp.clip(0.2 + 1 * jax.random.uniform(keys[10], (MOE_TOKENS, TOPK), jnp.float32) ** levels(keys[10], (MOE_TOKENS, TOPK), ((0, 8),), -0.2, 0.2), 0.2, 1.2)
    expert_gate = centred(keys[11], (EXPERTS * TP_GROUP, D, FF_DEV), D ** -0.5, 0.125, ((0, 32),))
    expert_up = centred(keys[12], (EXPERTS * TP_GROUP, D, FF_DEV), D ** -0.5, 0.125, ((0, 32),))
    expert_down = centred(keys[13], (EXPERTS * TP_GROUP, FF_DEV, D), FF ** -0.5, 0.1875, ((0, 32),))
    shared_gate = centred(keys[14], (D, FF_SHARED), D ** -0.5, 0.125, ((1, 4),))
    shared_up = centred(keys[15], (D, FF_SHARED), D ** -0.5, 0.125, ((1, 4),))
    shared_down = centred(keys[16], (FF_SHARED, D), FF_SHARED ** -0.5, 0.25, ((0, 4),))
    return dict(queries=queries, key_vectors=key_vectors, values=values, out_gate=out_gate, input_gate=input_gate, forget_gate=forget_gate, mix_weight=mix_weight, expert_input=expert_input, norm_gain=norm_gain, route_ids=route_ids, route_weights=route_weights, expert_gate=expert_gate, expert_up=expert_up, expert_down=expert_down, shared_gate=shared_gate, shared_up=shared_up, shared_down=shared_down)


epsilon = 1e-06
den_floor = 4.0

def mixer_part(queries, key_vectors, values, out_gate, input_gate, forget_gate, mix_weight):
    length = queries.shape[0]
    blocks = length // BLOCK
    factor = KEY_DIM ** (-0.5)
    causal = jnp.tril(jnp.ones((BLOCK, BLOCK), dtype=bool))

    def by_head(matrix, columns):
        return matrix.reshape(blocks, BLOCK, MEMORY_HEADS, columns).transpose(0, 2, 1, 3)
    query_blocks = by_head(queries, KEY_DIM)
    key_blocks = by_head(key_vectors, KEY_DIM)
    value_blocks = by_head(values, VAL_DIM)
    input_blocks = input_gate.reshape(blocks, BLOCK, MEMORY_HEADS).transpose(0, 2, 1)
    forget_blocks = jax.nn.log_sigmoid(forget_gate).reshape(blocks, BLOCK, MEMORY_HEADS).transpose(0, 2, 1)

    def block_step(carry_in, inputs):
        memory, normalizer, running = carry_in
        query_block, key_block, value_block, input_block, forget_block = inputs
        cumulative = jnp.cumsum(forget_block, axis=-1)
        carried = cumulative + running[:, None]
        log_weight = cumulative[:, :, None] - cumulative[:, None, :] + input_block[:, None, :]
        log_weight = jnp.where(causal, log_weight, -jnp.inf)
        stabilizer = jnp.maximum(carried, lax.optimization_barrier(jnp.max(log_weight, axis=-1)))
        within = jnp.exp(log_weight - stabilizer[:, :, None])
        across = jnp.exp(carried - stabilizer)
        query_wide = query_block.astype(jnp.float32)
        key_wide = key_block.astype(jnp.float32)
        value_wide = value_block.astype(jnp.float32)
        scores = jnp.einsum('htd,hsd->hts', query_wide, key_wide) * factor
        weights = scores * within
        weights_low = lax.optimization_barrier(weights.astype(jnp.bfloat16)).astype(jnp.float32)
        scaled = query_wide * factor
        numerator = across[:, :, None] * jnp.einsum('htd,hdv->htv', scaled, memory, precision=lax.Precision.HIGHEST)
        numerator = numerator + jnp.einsum('hts,hsv->htv', weights_low, value_wide)
        denominator = across * jnp.einsum('htd,hd->ht', scaled, normalizer, precision=lax.Precision.HIGHEST)
        denominator = denominator + lax.optimization_barrier(jnp.sum(weights, axis=-1))
        hidden = numerator / jnp.maximum(jnp.abs(denominator), den_floor)[:, :, None]
        block_total = cumulative[:, -1]
        log_retention = block_total[:, None] - cumulative + input_block
        running_next = jnp.maximum(block_total + running, lax.optimization_barrier(jnp.max(log_retention, axis=-1)))
        carry_decay = jnp.exp(block_total + running - running_next)
        weighted_keys = key_wide * jnp.exp(log_retention - running_next[:, None])[:, :, None]
        memory = carry_decay[:, None, None] * memory + jnp.einsum('hsd,hsv->hdv', weighted_keys, value_wide, precision=lax.Precision.HIGHEST)
        normalizer = carry_decay[:, None] * normalizer + lax.optimization_barrier(jnp.sum(weighted_keys, axis=1))
        return ((memory, normalizer, running_next), hidden)
    initial = (jnp.zeros((MEMORY_HEADS, KEY_DIM, VAL_DIM), jnp.float32), jnp.zeros((MEMORY_HEADS, KEY_DIM), jnp.float32), jnp.zeros((MEMORY_HEADS,), jnp.float32))
    _, hidden = lax.scan(block_step, initial, (query_blocks, key_blocks, value_blocks, input_blocks, forget_blocks))
    hidden = hidden.transpose(0, 2, 1, 3).reshape(length, MEMORY_HEADS * VAL_DIM)
    gated_rows = (hidden * jax.nn.sigmoid(out_gate.astype(jnp.float32))).astype(jnp.bfloat16)

    def add_group(summed, group_index):
        offset = (group_index * VAL_DEV).astype(jnp.int32)
        partial_value = jnp.dot(lax.dynamic_slice_in_dim(gated_rows, offset, VAL_DEV, 1), lax.dynamic_slice_in_dim(mix_weight, offset, VAL_DEV, 0), preferred_element_type=jnp.float32)
        return (summed + lax.optimization_barrier(partial_value.astype(jnp.bfloat16)).astype(jnp.float32), None)
    summed, _ = lax.scan(add_group, jnp.zeros((length, D), jnp.float32), jnp.arange(N_TP, dtype=jnp.int32))
    return summed.astype(jnp.bfloat16)

def expert_part(expert_input, norm_gain, route_ids, route_weights, expert_gate, expert_up, expert_down, shared_gate, shared_up, shared_down):
    rows_wide = expert_input.astype(jnp.float32)
    normed = (rows_wide * lax.rsqrt(lax.optimization_barrier(jnp.mean(rows_wide * rows_wide, axis=-1, keepdims=True)) + epsilon) * norm_gain).astype(jnp.bfloat16)
    chosen = route_ids.reshape(N_EP, MOE_DEV * TOPK)
    onehot = (chosen[:, :, None] == jnp.arange(EXPERTS, dtype=jnp.int32)[None, None, :]).astype(jnp.int32)
    earlier = jnp.cumsum(onehot, axis=1) - onehot
    slot_rank = lax.optimization_barrier(jnp.sum(earlier * onehot, axis=2))
    slot_index = (jnp.arange(N_EP, dtype=jnp.int32)[:, None] * CAP + slot_rank).reshape(-1)
    expert_of = route_ids.reshape(-1)
    token_of = jnp.arange(MOE_TOKENS * TOPK, dtype=jnp.int32) // TOPK
    slot_token = jnp.zeros((EXPERTS, N_EP * CAP), jnp.int32).at[expert_of, slot_index].set(token_of)
    slot_weight = jnp.zeros((EXPERTS, N_EP * CAP), jnp.float32).at[expert_of, slot_index].set(route_weights.reshape(-1))

    def one_expert(routed, expert_index):
        tokens_here = slot_token[expert_index]
        weight_here = slot_weight[expert_index]
        picked = normed[tokens_here].astype(jnp.float32)
        rows_base = (expert_index * TP_GROUP).astype(jnp.int32)
        gate_w = lax.dynamic_slice_in_dim(expert_gate, rows_base, TP_GROUP, 0).astype(jnp.float32)
        up_w = lax.dynamic_slice_in_dim(expert_up, rows_base, TP_GROUP, 0).astype(jnp.float32)
        down_w = lax.dynamic_slice_in_dim(expert_down, rows_base, TP_GROUP, 0).astype(jnp.float32)
        gate_val = jnp.einsum('rd,gdf->rgf', picked, gate_w)
        up_val = jnp.einsum('rd,gdf->rgf', picked, up_w)
        hidden = lax.optimization_barrier((jax.nn.silu(gate_val) * up_val).astype(jnp.bfloat16)).astype(jnp.float32)
        partials = jnp.einsum('rgf,gfd->rgd', hidden, down_w)
        partials = lax.optimization_barrier(partials.astype(jnp.bfloat16)).astype(jnp.float32)
        result = lax.optimization_barrier(jnp.sum(partials, axis=1)) * weight_here[:, None]
        return (routed.at[tokens_here].add(result), None)
    routed, _ = lax.scan(one_expert, jnp.zeros((MOE_TOKENS, D), jnp.float32), jnp.arange(EXPERTS, dtype=jnp.int32))
    shared_gate_val = jnp.dot(normed, shared_gate, preferred_element_type=jnp.float32)
    shared_up_val = jnp.dot(normed, shared_up, preferred_element_type=jnp.float32)
    shared_act = (jax.nn.silu(shared_gate_val) * shared_up_val).astype(jnp.bfloat16)
    shared_rows = jnp.dot(shared_act, shared_down, preferred_element_type=jnp.float32)
    return (routed + shared_rows).astype(jnp.bfloat16)

def reference(queries, key_vectors, values, out_gate, input_gate, forget_gate, mix_weight, expert_input, norm_gain, route_ids, route_weights, expert_gate, expert_up, expert_down, shared_gate, shared_up, shared_down):
    mixer_out = mixer_part(queries, key_vectors, values, out_gate, input_gate, forget_gate, mix_weight)
    expert_out = expert_part(expert_input, norm_gain, route_ids, route_weights, expert_gate, expert_up, expert_down, shared_gate, shared_up, shared_down)
    return (mixer_out, expert_out)
```

```python
import jax
import jax.numpy as jnp
from jax import lax
from jax.sharding import PartitionSpec as P

D = 2048
MEMORY_HEADS = 2
KEY_DIM = 256
BLOCK = 128
FF = 1024


epsilon = 1e-06
lowest = -1e30
den_floor = 4.0


def mixer_half(queries, key_vectors, values, out_gate, input_gate, forget_gate, mix_weight):
    tp_count = lax.axis_size("tp")
    tp_rank = lax.axis_index("tp")
    ep_count = lax.axis_size("ep")
    ep_rank = lax.axis_index("ep")
    length = queries.shape[0]
    channels = values.shape[1]
    factor = KEY_DIM ** (-0.5)
    head_index = tp_rank // (tp_count // MEMORY_HEADS)
    offset = head_index * KEY_DIM
    query_head = lax.dynamic_slice_in_dim(queries, offset, KEY_DIM, 1)
    key_head = lax.dynamic_slice_in_dim(key_vectors, offset, KEY_DIM, 1)
    both = lax.all_gather(jnp.concatenate([key_head, values], axis=1), "ep", axis=0, tiled=True)
    keys_all = both[:, :KEY_DIM]
    values_all = both[:, KEY_DIM:]
    select = jnp.arange(MEMORY_HEADS, dtype=jnp.int32)[None, :] == head_index
    gates = jnp.stack(
        [
            jnp.sum(jnp.where(select, input_gate, 0.0), axis=1),
            jax.nn.log_sigmoid(jnp.sum(jnp.where(select, forget_gate, 0.0), axis=1)),
        ]
    )
    gates = lax.all_gather(gates, "ep", axis=1, tiled=True)
    total = ep_count * length
    blocks = total // BLOCK
    mine = length // BLOCK
    input_all = gates[0].reshape(blocks, BLOCK)
    cumulative = jnp.cumsum(gates[1].reshape(blocks, BLOCK), axis=1)
    block_total = cumulative[:, -1]
    index = jnp.arange(blocks, dtype=jnp.int32)
    here = ep_rank * mine + jnp.arange(mine, dtype=jnp.int32)
    between = (index[None, None, :] > index[None, :, None]) & (
        index[None, None, :] < here[:, None, None]
    )
    gap = jnp.sum(jnp.where(between, block_total[None, None, :], 0.0), axis=2)
    ahead = jnp.sum(jnp.where(index[None, :] < here[:, None], block_total[None, :], 0.0), axis=1)
    keep = block_total[:, None] - cumulative + input_all
    own_cumulative = lax.dynamic_slice_in_dim(cumulative, ep_rank * mine, mine, 0)
    same = index[None, :] == here[:, None]
    column = jnp.where(same[:, :, None], input_all - cumulative, keep + gap[:, :, None])
    log_weight = own_cumulative[:, :, None, None] + column[:, None]
    row_at = jnp.arange(BLOCK, dtype=jnp.int32)
    visible = (index[None, :] < here[:, None])[:, None, :, None] | (
        same[:, None, :, None] & (row_at[None, :, None, None] >= row_at[None, None, None, :])
    )
    log_weight = jnp.where(visible, log_weight, -jnp.inf).reshape(length, total)
    carried = (own_cumulative + ahead[:, None]).reshape(length)
    stabilizer = jnp.maximum(carried, jnp.max(log_weight, axis=1))
    within = jnp.exp(log_weight - stabilizer[:, None])
    scores = (
        jnp.einsum("td,sd->ts", query_head, keys_all, preferred_element_type=jnp.float32) * factor
    )
    weights = scores * within
    numerator = jnp.dot(
        weights.astype(jnp.bfloat16), values_all, preferred_element_type=jnp.float32
    )
    denominator = jnp.sum(weights, axis=1)
    hidden = numerator / jnp.maximum(jnp.abs(denominator), den_floor)[:, None]
    gated_rows = (hidden * jax.nn.sigmoid(out_gate.astype(jnp.float32))).astype(jnp.bfloat16)
    return jnp.dot(gated_rows, mix_weight, preferred_element_type=jnp.float32)


def dense_experts(
    expert_input,
    norm_gain,
    route_ids,
    route_weights,
    expert_gate,
    expert_up,
    expert_down,
    shared_gate,
    shared_up,
    shared_down,
):
    ep_count = lax.axis_size("ep")
    tp_count = lax.axis_size("tp")
    tp_rank = lax.axis_index("tp")
    ep_rank = lax.axis_index("ep")
    tokens = expert_input.shape[0]
    share = tokens // tp_count
    rows_wide = expert_input.astype(jnp.float32)
    normed = (
        rows_wide
        * lax.rsqrt(jnp.mean(rows_wide * rows_wide, axis=-1, keepdims=True) + epsilon)
        * norm_gain
    ).astype(jnp.bfloat16)
    part = lax.dynamic_slice_in_dim(normed, tp_rank * share, share, 0)
    everyone = lax.all_gather(part, ("ep", "tp"), axis=0, tiled=True)
    named = route_ids[:, :, None] == jnp.arange(ep_count, dtype=jnp.int32)[None, None, :]
    table = jnp.sum(jnp.where(named, route_weights[:, :, None], 0.0), axis=1).T
    table = lax.all_to_all(table, "ep", split_axis=0, concat_axis=1, tiled=True)
    mine = table.reshape(ep_count * tokens)
    gate_val = jnp.dot(everyone, expert_gate[0], preferred_element_type=jnp.float32)
    up_val = jnp.dot(everyone, expert_up[0], preferred_element_type=jnp.float32)
    hidden = (jax.nn.silu(gate_val) * up_val).astype(jnp.bfloat16)
    partial_value = jnp.dot(hidden, expert_down[0], preferred_element_type=jnp.float32)
    partial_value = (partial_value * mine[:, None]).astype(jnp.bfloat16)
    routed = lax.psum_scatter(partial_value, ("ep", "tp"), scatter_dimension=0, tiled=True)
    shared_gate_val = jnp.dot(normed, shared_gate, preferred_element_type=jnp.float32)
    shared_up_val = jnp.dot(normed, shared_up, preferred_element_type=jnp.float32)
    shared_act = (jax.nn.silu(shared_gate_val) * shared_up_val).astype(jnp.bfloat16)
    shared = jnp.dot(shared_act, shared_down, preferred_element_type=jnp.float32)
    shared = lax.psum_scatter(
        shared.astype(jnp.bfloat16), "tp", scatter_dimension=0, tiled=True
    )
    piece = (routed.astype(jnp.float32) + shared.astype(jnp.float32)).astype(jnp.bfloat16)
    return lax.all_gather(piece, "tp", axis=0, tiled=True)


def expert_half(
    expert_input,
    norm_gain,
    route_ids,
    route_weights,
    expert_gate,
    expert_up,
    expert_down,
    shared_gate,
    shared_up,
    shared_down,
):
    ep_count = lax.axis_size("ep")
    tp_count = lax.axis_size("tp")
    tp_rank = lax.axis_index("tp")
    tokens = expert_input.shape[0]
    top_count = route_ids.shape[1]
    slice_units = expert_gate.shape[2]
    group_size = FF // slice_units
    per_ep = tp_count // group_size
    team_index = tp_rank // group_size
    expert_count = ep_count * per_ep
    capacity = 2 * tokens * top_count // expert_count
    rows_wide = expert_input.astype(jnp.float32)
    normed = (
        rows_wide
        * lax.rsqrt(jnp.mean(rows_wide * rows_wide, axis=-1, keepdims=True) + epsilon)
        * norm_gain
    ).astype(jnp.bfloat16)
    chosen = route_ids.reshape(-1)
    onehot = (chosen[:, None] == jnp.arange(expert_count, dtype=jnp.int32)[None, :]).astype(
        jnp.int32
    )
    slot_rank = jnp.sum((jnp.cumsum(onehot, axis=0) - onehot) * onehot, axis=1)
    in_team = chosen % per_ep == team_index
    target = jnp.where(in_team, chosen // per_ep * capacity + slot_rank, ep_count * capacity)
    token_of = jnp.arange(chosen.shape[0], dtype=jnp.int32) // top_count
    slot_token = jnp.zeros((ep_count * capacity,), jnp.int32).at[target].set(token_of, mode="drop")
    slot_live = jnp.zeros((ep_count * capacity,), jnp.int32).at[target].set(1, mode="drop")
    outgoing = jnp.where(slot_live[:, None] > 0, normed[slot_token], jnp.zeros((), jnp.bfloat16))
    outgoing = outgoing.reshape(ep_count, capacity, D)
    gate_slice = expert_gate[0]
    up_slice = expert_up[0]
    down_slice = expert_down[0]
    arrived = lax.all_to_all(outgoing, "ep", split_axis=0, concat_axis=0, tiled=True)
    gate_val = jnp.einsum("sid,df->sif", arrived, gate_slice, preferred_element_type=jnp.float32)
    up_val = jnp.einsum("sid,df->sif", arrived, up_slice, preferred_element_type=jnp.float32)
    hidden = (jax.nn.silu(gate_val) * up_val).astype(jnp.bfloat16)
    partial_value = jnp.einsum(
        "sif,fd->sid", hidden, down_slice, preferred_element_type=jnp.float32
    )
    partial_value = partial_value.astype(jnp.bfloat16)
    returned = lax.all_to_all(partial_value, "ep", split_axis=0, concat_axis=0, tiled=True)
    flat_back = returned.reshape(ep_count * capacity, returned.shape[2])
    gather_at = jnp.where(in_team, target, 0).reshape(tokens, top_count)
    weight_at = jnp.where(in_team, route_weights.reshape(-1), 0.0).reshape(tokens, top_count)
    combined = jnp.zeros((tokens, returned.shape[2]), jnp.float32)
    for pick_index in range(top_count):
        combined = (
            combined
            + flat_back[gather_at[:, pick_index]].astype(jnp.float32)
            * weight_at[:, pick_index][:, None]
        )
    shared_gate_val = jnp.dot(normed, shared_gate, preferred_element_type=jnp.float32)
    shared_up_val = jnp.dot(normed, shared_up, preferred_element_type=jnp.float32)
    shared_act = (jax.nn.silu(shared_gate_val) * shared_up_val).astype(jnp.bfloat16)
    return combined + jnp.dot(shared_act, shared_down, preferred_element_type=jnp.float32)


def shards(
    queries,
    key_vectors,
    values,
    out_gate,
    input_gate,
    forget_gate,
    mix_weight,
    expert_input,
    norm_gain,
    route_ids,
    route_weights,
    expert_gate,
    expert_up,
    expert_down,
    shared_gate,
    shared_up,
    shared_down,
):
    ep_count, tp_count = lax.axis_size("ep"), lax.axis_size("tp")
    tokens, slots = expert_input.shape[0], route_ids.shape[1] * 2 * expert_input.shape[0]
    per_ep = tp_count * expert_gate.shape[2] // FF
    dense = per_ep == 1 and slots // (ep_count * per_ep) >= tokens
    mixer_partial = mixer_half(
        queries, key_vectors, values, out_gate, input_gate, forget_gate, mix_weight
    )
    experts = dense_experts if dense else expert_half
    expert_partial = experts(
        expert_input,
        norm_gain,
        route_ids,
        route_weights,
        expert_gate,
        expert_up,
        expert_down,
        shared_gate,
        shared_up,
        shared_down,
    )
    mixer_piece = lax.psum_scatter(
        mixer_partial.astype(jnp.bfloat16), "tp", scatter_dimension=0, tiled=True
    )
    mixer_out = lax.all_gather(mixer_piece, "tp", axis=0, tiled=True)
    if dense:
        return (mixer_out, expert_partial)
    expert_piece = lax.psum_scatter(expert_partial, "tp", scatter_dimension=0, tiled=True).astype(
        jnp.bfloat16
    )
    expert_out = lax.all_gather(expert_piece, "tp", axis=0, tiled=True)
    return (mixer_out, expert_out)


def solution(mesh):
    return jax.shard_map(
        shards,
        mesh=mesh,
        in_specs=(
            P("ep", None),
            P("ep", None),
            P("ep", "tp"),
            P("ep", "tp"),
            P("ep", None),
            P("ep", None),
            P("tp", None),
            P("ep", None),
            P(),
            P("ep", None),
            P("ep", None),
            P(("ep", "tp"), None, None),
            P(("ep", "tp"), None, None),
            P(("ep", "tp"), None, None),
            P(None, "tp"),
            P(None, "tp"),
            P("tp", None),
        ),
        out_specs=(P("ep", None), P("ep", None)),
        check_vma=False,
    )
```

```python
import functools

import jax
import jax.numpy as jnp
from jax import lax
from jax.experimental import pallas as pl
from jax.experimental.pallas import tpu as pltpu
from jax.sharding import PartitionSpec as P

D = 2048
MEMORY_HEADS = 2
KEY_DIM = 256
BLOCK = 128
FF = 1024


epsilon = 1e-06
lowest = -1e30
den_floor = 4.0


def mixer_half(queries, key_vectors, values, out_gate, input_gate, forget_gate, mix_weight):
    tp_count = lax.axis_size("tp")
    tp_rank = lax.axis_index("tp")
    ep_count = lax.axis_size("ep")
    ep_rank = lax.axis_index("ep")
    length = queries.shape[0]
    channels = values.shape[1]
    factor = KEY_DIM ** (-0.5)
    head_index = tp_rank // (tp_count // MEMORY_HEADS)
    offset = head_index * KEY_DIM
    query_head = lax.dynamic_slice_in_dim(queries, offset, KEY_DIM, 1)
    key_head = lax.dynamic_slice_in_dim(key_vectors, offset, KEY_DIM, 1)
    both = lax.all_gather(jnp.concatenate([key_head, values], axis=1), "ep", axis=0, tiled=True)
    keys_all = both[:, :KEY_DIM]
    values_all = both[:, KEY_DIM:]
    select = jnp.arange(MEMORY_HEADS, dtype=jnp.int32)[None, :] == head_index
    gates = jnp.stack(
        [
            jnp.sum(jnp.where(select, input_gate, 0.0), axis=1),
            jax.nn.log_sigmoid(jnp.sum(jnp.where(select, forget_gate, 0.0), axis=1)),
        ]
    )
    gates = lax.all_gather(gates, "ep", axis=1, tiled=True)
    total = ep_count * length
    blocks = total // BLOCK
    mine = length // BLOCK
    input_all = gates[0].reshape(blocks, BLOCK)
    cumulative = jnp.cumsum(gates[1].reshape(blocks, BLOCK), axis=1)
    block_total = cumulative[:, -1]
    index = jnp.arange(blocks, dtype=jnp.int32)
    here = ep_rank * mine + jnp.arange(mine, dtype=jnp.int32)
    between = (index[None, None, :] > index[None, :, None]) & (
        index[None, None, :] < here[:, None, None]
    )
    gap = jnp.sum(jnp.where(between, block_total[None, None, :], 0.0), axis=2)
    ahead = jnp.sum(jnp.where(index[None, :] < here[:, None], block_total[None, :], 0.0), axis=1)
    keep = block_total[:, None] - cumulative + input_all
    own_cumulative = lax.dynamic_slice_in_dim(cumulative, ep_rank * mine, mine, 0)
    same = index[None, :] == here[:, None]
    column = jnp.where(same[:, :, None], input_all - cumulative, keep + gap[:, :, None])
    log_weight = own_cumulative[:, :, None, None] + column[:, None]
    row_at = jnp.arange(BLOCK, dtype=jnp.int32)
    visible = (index[None, :] < here[:, None])[:, None, :, None] | (
        same[:, None, :, None] & (row_at[None, :, None, None] >= row_at[None, None, None, :])
    )
    log_weight = jnp.where(visible, log_weight, -jnp.inf).reshape(length, total)
    carried = (own_cumulative + ahead[:, None]).reshape(length)
    stabilizer = jnp.maximum(carried, jnp.max(log_weight, axis=1))
    within = jnp.exp(log_weight - stabilizer[:, None])
    scores = (
        jnp.einsum("td,sd->ts", query_head, keys_all, preferred_element_type=jnp.float32) * factor
    )
    weights = scores * within
    numerator = jnp.dot(
        weights.astype(jnp.bfloat16), values_all, preferred_element_type=jnp.float32
    )
    denominator = jnp.sum(weights, axis=1)
    hidden = numerator / jnp.maximum(jnp.abs(denominator), den_floor)[:, None]
    gated_rows = (hidden * jax.nn.sigmoid(out_gate.astype(jnp.float32))).astype(jnp.bfloat16)
    return gated_rows


def dense_kernel(
    lines, teams, x_ref, wt_ref, sact_ref, gated_ref, g_ref, u_ref, d_ref, sd_ref, mw_ref,
    eo_ref, mo_ref,
    tok, act, dq, sdq, mwq, sall, gall, xout, xin, own, zout, zin, fin, mfin,
    z_send, z_recv, x_send, x_recv, c_send, c_recv, a_send, a_recv,
    w_send, w_recv, xo_send, xo_recv, zo_send, zo_recv, f_send, f_recv,
):
    me = lax.axis_index("ep")
    j = lax.axis_index("tp")
    z, x = me // 2, me % 2
    half_rows = x_ref.shape[0] // 2
    core = j % 2
    buddy = j + 1 - 2 * core
    quarter = fin.shape[2]
    mine_rows = pl.ds(pl.multiple_of(core * half_rows, half_rows), half_rows)
    other_rows = pl.ds(pl.multiple_of((1 - core) * half_rows, half_rows), half_rows)

    def remote(src, dst, send, recv, ep, tp):
        return pltpu.make_async_remote_copy(
            src_ref=src, dst_ref=dst, send_sem=send, recv_sem=recv,
            device_id={"ep": ep, "tp": tp}, device_id_type=pl.DeviceIdType.MESH,
        )

    barrier = pltpu.get_barrier_semaphore()

    def greet(ep, tp):
        pl.semaphore_signal(
            barrier, inc=1, device_id={"ep": ep, "tp": tp}, device_id_type=pl.DeviceIdType.MESH
        )

    greet(z * 2 + 1 - x, j)
    for k in range(1, lines):
        greet(lax.rem(z + k, lines) * 2 + x, j)
    for k in range(1, teams):
        greet(me, lax.rem(j + k, teams))
    pl.semaphore_wait(barrier, lines + teams - 1)

    def columns(ref, q):
        return ref.at[:, pl.ds(pl.multiple_of(q * quarter, quarter), quarter)]

    def team_copies(k):
        p = lax.rem(j + k, teams)
        pairs = (
            (sact_ref, sall.at[j]),
            (columns(sd_ref, p), sdq.at[j]),
            (gated_ref, gall.at[j]),
            (columns(mw_ref, p), mwq.at[j]),
            (columns(d_ref, p), dq.at[j]),
        )
        return [
            remote(src, dst, w_send.at[n, k - 1], w_recv.at[n, k - 1], me, p)
            for n, (src, dst) in enumerate(pairs)
        ]

    def z_copy(zb, way):
        to = z + 1 - 2 * way
        ref = tok.at[zb * 2 + x, mine_rows]
        return remote(ref, ref, z_send.at[way, zb], z_recv.at[zb], to * 2 + x, j)

    def x_copy(zb):
        ref = tok.at[zb * 2 + x, mine_rows]
        return remote(ref, ref, x_send.at[zb], x_recv.at[zb], z * 2 + 1 - x, j)

    def x_arrival(zb):
        ref = tok.at[zb * 2 + 1 - x, mine_rows]
        return remote(ref, ref, x_send.at[zb], x_recv.at[zb], z * 2 + 1 - x, j)

    def c_copy(block):
        ref = tok.at[block, mine_rows]
        return remote(ref, ref, c_send.at[block], c_recv.at[block], me, buddy)

    def c_arrival(block):
        ref = tok.at[block, other_rows]
        return remote(ref, ref, c_send.at[block], c_recv.at[block], me, buddy)

    def a_copy(block, k):
        p = lax.rem(j + k, teams)
        return remote(
            act.at[block, j], act.at[block, j],
            a_send.at[block, k - 1], a_recv.at[block, k - 1], me, p,
        )

    def a_arrival(block, k):
        p = lax.rem(j + teams - k, teams)
        return remote(
            act.at[block, p], act.at[block, p],
            a_send.at[block, k - 1], a_recv.at[block, k - 1], me, p,
        )

    tok[me] = x_ref[...]
    for way in range(2):
        to = z + 1 - 2 * way

        @pl.when((to >= 0) & (to < lines))
        def _():
            remote(
                x_ref.at[mine_rows], tok.at[me, mine_rows],
                z_send.at[way, z], z_recv.at[z], to * 2 + x, j,
            ).start()

    remote(
        x_ref.at[mine_rows], tok.at[me, mine_rows], x_send.at[z], x_recv.at[z], z * 2 + 1 - x, j
    ).start()
    for k in range(1, teams):
        for copy in team_copies(k):
            copy.start()
    sall[j] = sact_ref[...]
    gall[j] = gated_ref[...]
    sdq[j] = columns(sd_ref, j)[...]
    mwq[j] = columns(mw_ref, j)[...]
    dq[j] = columns(d_ref, j)[...]

    def forward(zb, d):
        z_copy(zb, d).wait_recv()
        to = z + 1 - 2 * d

        @pl.when((to >= 0) & (to < lines))
        def _():
            z_copy(zb, d).start()

        x_copy(zb).start()
        c_copy(zb * 2 + x).start()

    def activate(block):
        rows = tok[block]
        gate = jnp.dot(rows, g_ref[...], preferred_element_type=jnp.float32)
        up = jnp.dot(rows, u_ref[...], preferred_element_type=jnp.float32)
        act[block, j] = (gate / (1.0 + jnp.exp(-gate)) * up).astype(jnp.bfloat16)
        for k in range(1, teams):
            a_copy(block, k).start()

    def finish(block):
        for k in range(1, teams):
            a_arrival(block, k).wait_recv()
        total = jnp.dot(act[block, 0], dq[0], preferred_element_type=jnp.float32)
        for q in range(1, teams):
            total += jnp.dot(act[block, q], dq[q], preferred_element_type=jnp.float32)
        return (total * wt_ref[block]).astype(jnp.bfloat16)

    def xo_copy(zb):
        return remote(
            xout.at[zb], xin.at[zb], xo_send.at[zb], xo_recv.at[zb], z * 2 + 1 - x, j
        )

    def zo_copy(zb):
        return remote(
            zout.at[zb], zin.at[z], zo_send.at[zb], zo_recv.at[z], zb * 2 + x, j
        )

    def zo_arrival(zb):
        return remote(
            zout.at[zb], zin.at[zb], zo_send.at[zb], zo_recv.at[zb], zb * 2 + x, j
        )

    def valid(s, d, zb):
        return (s >= 0) & (s < lines) & (zb >= 0) & (zb < lines) & ((s > 0) | (d == 0))

    def step(t, carry):
        def stage_one(d, carry):
            s = t
            zb = z + s * (2 * d - 1)

            @pl.when(valid(s, d, zb) & (s > 0))
            def _():
                forward(zb, d)

            return carry

        lax.fori_loop(0, 2, stage_one, 0)

        def stage_two(d, carry):
            s = t - 1
            zb = z + s * (2 * d - 1)

            @pl.when(valid(s, d, zb))
            def _():
                x_arrival(zb).wait_recv()
                c_copy(zb * 2 + 1 - x).start()

                def column(n, carry):
                    block = zb * 2 + lax.rem(x + n, 2)

                    @pl.when(block != me)
                    def _():
                        c_arrival(block).wait_recv()

                    activate(block)
                    return carry

                lax.fori_loop(0, 2, column, 0)

            return carry

        lax.fori_loop(0, 2, stage_two, 0)

        @pl.when(t == 2)
        def _():
            for k in range(1, teams):
                for copy in team_copies(k):
                    copy.wait_recv()

        def stage_three(d, carry):
            s = t - 2
            zb = z + s * (2 * d - 1)

            @pl.when(valid(s, d, zb))
            def _():
                xout[zb] = finish(zb * 2 + 1 - x)
                xo_copy(zb).start()
                own[zb] = finish(zb * 2 + x)

            return carry

        lax.fori_loop(0, 2, stage_three, 0)

        def stage_four(d, carry):
            s = t - 3
            zb = z + s * (2 * d - 1)

            @pl.when(valid(s, d, zb))
            def _():
                xo_copy(zb).wait_recv()

                @pl.when(s > 0)
                def _():
                    zout[zb] = (
                        own[zb].astype(jnp.float32) + xin[zb].astype(jnp.float32)
                    ).astype(jnp.bfloat16)
                    zo_copy(zb).start()

            return carry

        lax.fori_loop(0, 2, stage_four, 0)
        return carry

    lax.fori_loop(1, lines + 3, step, 0)

    def f_copies(k, source, rows):
        p = lax.rem(j + k, teams)
        return remote(
            rows.at[source], rows.at[source],
            f_send.at[0 if rows is fin else 1, k - 1], f_recv.at[0 if rows is fin else 1, k - 1],
            me, p,
        )

    mixed = jnp.zeros(mfin.shape[1:], jnp.float32)
    for q in range(teams):
        mixed += (
            jnp.dot(gall[q], mwq[q], preferred_element_type=jnp.float32)
            .astype(jnp.bfloat16)
            .astype(jnp.float32)
        )
    mfin[j] = mixed.astype(jnp.bfloat16)
    for k in range(1, teams):
        f_copies(k, j, mfin).start()

    total = own[z].astype(jnp.float32) + xin[z].astype(jnp.float32)
    for q in range(teams):
        total += jnp.dot(sall[q], sdq[q], preferred_element_type=jnp.float32)
    for k in range(1, lines):
        source = lax.rem(z + k, lines)
        zo_arrival(source).wait_recv()
        total += zin[source].astype(jnp.float32)
    fin[j] = total.astype(jnp.bfloat16)
    for k in range(1, teams):
        f_copies(k, j, fin).start()
    for rows in (mfin, fin):
        for k in range(1, teams):
            f_copies(k, lax.rem(j + teams - k, teams), rows).wait_recv()
    for q in range(teams):
        mo_ref[:, q * quarter : (q + 1) * quarter] = mfin[q]
        eo_ref[:, q * quarter : (q + 1) * quarter] = fin[q]

    for k in range(1, teams):
        f_copies(k, j, mfin).wait_send()
        f_copies(k, j, fin).wait_send()
        for copy in team_copies(k):
            copy.wait_send()

    def drain(zb, carry):
        for way in range(2):
            to = z + 1 - 2 * way
            passing = (zb <= z) if way == 0 else (zb >= z)

            @pl.when((to >= 0) & (to < lines) & passing)
            def _():
                z_copy(zb, way).wait_send()

        x_copy(zb).wait_send()
        xo_copy(zb).wait_send()

        @pl.when(zb != z)
        def _():
            zo_copy(zb).wait_send()

        def column(n, carry):
            block = zb * 2 + n

            @pl.when(block != me)
            def _():
                c_copy(block).wait_send()

            for k in range(1, teams):
                a_copy(block, k).wait_send()
            return carry

        lax.fori_loop(0, 2, column, 0)
        return carry

    lax.fori_loop(0, lines, drain, 0)


def dense_experts(
    gated_rows,
    mix_weight,
    expert_input,
    norm_gain,
    route_ids,
    route_weights,
    expert_gate,
    expert_up,
    expert_down,
    shared_gate,
    shared_up,
    shared_down,
):
    ep_count = lax.axis_size("ep")
    teams = lax.axis_size("tp")
    lines = ep_count // 2
    tokens, width = expert_input.shape
    quarter = width // teams
    units = expert_gate.shape[2]
    shared_units = shared_gate.shape[1]
    length, channels = gated_rows.shape
    rows_wide = expert_input.astype(jnp.float32)
    normed = (
        rows_wide
        * lax.rsqrt(jnp.mean(rows_wide * rows_wide, axis=-1, keepdims=True) + epsilon)
        * norm_gain
    ).astype(jnp.bfloat16)
    named = route_ids[:, :, None] == jnp.arange(ep_count, dtype=jnp.int32)[None, None, :]
    table = jnp.sum(jnp.where(named, route_weights[:, :, None], 0.0), axis=1).T
    table = lax.all_to_all(table, "ep", split_axis=0, concat_axis=1, tiled=True)
    table = table.reshape(ep_count, tokens, 1)
    shared_gate_val = jnp.dot(normed, shared_gate, preferred_element_type=jnp.float32)
    shared_up_val = jnp.dot(normed, shared_up, preferred_element_type=jnp.float32)
    shared_act = (jax.nn.silu(shared_gate_val) * shared_up_val).astype(jnp.bfloat16)
    low, dma = jnp.bfloat16, pltpu.SemaphoreType.DMA
    vmem = pl.BlockSpec(memory_space=pltpu.VMEM)
    expert_out, mixer_out = pl.pallas_call(
        functools.partial(dense_kernel, lines, teams),
        out_shape=(
            jax.ShapeDtypeStruct((tokens, width), low),
            jax.ShapeDtypeStruct((length, width), low),
        ),
        in_specs=[vmem] * 9,
        out_specs=(vmem, vmem),
        scratch_shapes=[
            pltpu.VMEM((ep_count, tokens, width), low),
            pltpu.VMEM((ep_count, teams, tokens, units), low),
            pltpu.VMEM((teams, units, quarter), low),
            pltpu.VMEM((teams, shared_units, quarter), low),
            pltpu.VMEM((teams, channels, quarter), low),
            pltpu.VMEM((teams, tokens, shared_units), low),
            pltpu.VMEM((teams, length, channels), low),
            pltpu.VMEM((lines, tokens, quarter), low),
            pltpu.VMEM((lines, tokens, quarter), low),
            pltpu.VMEM((lines, tokens, quarter), low),
            pltpu.VMEM((lines, tokens, quarter), low),
            pltpu.VMEM((lines, tokens, quarter), low),
            pltpu.VMEM((teams, tokens, quarter), low),
            pltpu.VMEM((teams, length, quarter), low),
            dma((2, lines)), dma((lines,)), dma((lines,)), dma((lines,)),
            dma((ep_count,)), dma((ep_count,)),
            dma((ep_count, teams - 1)), dma((ep_count, teams - 1)),
            dma((5, teams - 1)), dma((5, teams - 1)),
            dma((lines,)), dma((lines,)), dma((lines,)), dma((lines,)),
            dma((2, teams - 1)), dma((2, teams - 1)),
        ],
        compiler_params=pltpu.CompilerParams(
            collective_id=0, has_side_effects=True, vmem_limit_bytes=56 * 1024 * 1024
        ),
    )(
        normed, table, shared_act, gated_rows,
        expert_gate[0], expert_up[0], expert_down[0], shared_down, mix_weight,
    )
    return mixer_out, expert_out


def expert_half(
    expert_input,
    norm_gain,
    route_ids,
    route_weights,
    expert_gate,
    expert_up,
    expert_down,
    shared_gate,
    shared_up,
    shared_down,
):
    ep_count = lax.axis_size("ep")
    tp_count = lax.axis_size("tp")
    tp_rank = lax.axis_index("tp")
    tokens = expert_input.shape[0]
    top_count = route_ids.shape[1]
    slice_units = expert_gate.shape[2]
    group_size = FF // slice_units
    per_ep = tp_count // group_size
    team_index = tp_rank // group_size
    expert_count = ep_count * per_ep
    capacity = 2 * tokens * top_count // expert_count
    rows_wide = expert_input.astype(jnp.float32)
    normed = (
        rows_wide
        * lax.rsqrt(jnp.mean(rows_wide * rows_wide, axis=-1, keepdims=True) + epsilon)
        * norm_gain
    ).astype(jnp.bfloat16)
    chosen = route_ids.reshape(-1)
    onehot = (chosen[:, None] == jnp.arange(expert_count, dtype=jnp.int32)[None, :]).astype(
        jnp.int32
    )
    slot_rank = jnp.sum((jnp.cumsum(onehot, axis=0) - onehot) * onehot, axis=1)
    in_team = chosen % per_ep == team_index
    target = jnp.where(in_team, chosen // per_ep * capacity + slot_rank, ep_count * capacity)
    token_of = jnp.arange(chosen.shape[0], dtype=jnp.int32) // top_count
    slot_token = jnp.zeros((ep_count * capacity,), jnp.int32).at[target].set(token_of, mode="drop")
    slot_live = jnp.zeros((ep_count * capacity,), jnp.int32).at[target].set(1, mode="drop")
    outgoing = jnp.where(slot_live[:, None] > 0, normed[slot_token], jnp.zeros((), jnp.bfloat16))
    outgoing = outgoing.reshape(ep_count, capacity, D)
    gate_slice = expert_gate[0]
    up_slice = expert_up[0]
    down_slice = expert_down[0]
    arrived = lax.all_to_all(outgoing, "ep", split_axis=0, concat_axis=0, tiled=True)
    gate_val = jnp.einsum("sid,df->sif", arrived, gate_slice, preferred_element_type=jnp.float32)
    up_val = jnp.einsum("sid,df->sif", arrived, up_slice, preferred_element_type=jnp.float32)
    hidden = (jax.nn.silu(gate_val) * up_val).astype(jnp.bfloat16)
    partial_value = jnp.einsum(
        "sif,fd->sid", hidden, down_slice, preferred_element_type=jnp.float32
    )
    partial_value = partial_value.astype(jnp.bfloat16)
    returned = lax.all_to_all(partial_value, "ep", split_axis=0, concat_axis=0, tiled=True)
    flat_back = returned.reshape(ep_count * capacity, returned.shape[2])
    gather_at = jnp.where(in_team, target, 0).reshape(tokens, top_count)
    weight_at = jnp.where(in_team, route_weights.reshape(-1), 0.0).reshape(tokens, top_count)
    combined = jnp.zeros((tokens, returned.shape[2]), jnp.float32)
    for pick_index in range(top_count):
        combined = (
            combined
            + flat_back[gather_at[:, pick_index]].astype(jnp.float32)
            * weight_at[:, pick_index][:, None]
        )
    shared_gate_val = jnp.dot(normed, shared_gate, preferred_element_type=jnp.float32)
    shared_up_val = jnp.dot(normed, shared_up, preferred_element_type=jnp.float32)
    shared_act = (jax.nn.silu(shared_gate_val) * shared_up_val).astype(jnp.bfloat16)
    return combined + jnp.dot(shared_act, shared_down, preferred_element_type=jnp.float32)


def shards(
    queries,
    key_vectors,
    values,
    out_gate,
    input_gate,
    forget_gate,
    mix_weight,
    expert_input,
    norm_gain,
    route_ids,
    route_weights,
    expert_gate,
    expert_up,
    expert_down,
    shared_gate,
    shared_up,
    shared_down,
):
    ep_count, tp_count = lax.axis_size("ep"), lax.axis_size("tp")
    tokens, slots = expert_input.shape[0], route_ids.shape[1] * 2 * expert_input.shape[0]
    per_ep = tp_count * expert_gate.shape[2] // FF
    even = ep_count % 2 == 0 and tp_count % 2 == 0
    dense = even and per_ep == 1 and slots // (ep_count * per_ep) >= tokens
    gated_rows = mixer_half(
        queries, key_vectors, values, out_gate, input_gate, forget_gate, mix_weight
    )
    experts = (
        expert_input,
        norm_gain,
        route_ids,
        route_weights,
        expert_gate,
        expert_up,
        expert_down,
        shared_gate,
        shared_up,
        shared_down,
    )
    if dense:
        return dense_experts(gated_rows, mix_weight, *experts)
    mixer_partial = jnp.dot(gated_rows, mix_weight, preferred_element_type=jnp.float32)
    expert_partial = expert_half(*experts)
    mixer_piece = lax.psum_scatter(
        mixer_partial.astype(jnp.bfloat16), "tp", scatter_dimension=0, tiled=True
    )
    mixer_out = lax.all_gather(mixer_piece, "tp", axis=0, tiled=True)
    expert_piece = lax.psum_scatter(expert_partial, "tp", scatter_dimension=0, tiled=True).astype(
        jnp.bfloat16
    )
    expert_out = lax.all_gather(expert_piece, "tp", axis=0, tiled=True)
    return (mixer_out, expert_out)


def solution(mesh):
    return jax.shard_map(
        shards,
        mesh=mesh,
        in_specs=(
            P("ep", None),
            P("ep", None),
            P("ep", "tp"),
            P("ep", "tp"),
            P("ep", None),
            P("ep", None),
            P("tp", None),
            P("ep", None),
            P(),
            P("ep", None),
            P("ep", None),
            P(("ep", "tp"), None, None),
            P(("ep", "tp"), None, None),
            P(("ep", "tp"), None, None),
            P(None, "tp"),
            P(None, "tp"),
            P("tp", None),
        ),
        out_specs=(P("ep", None), P("ep", None)),
        check_vma=False,
    )
```

```python
import functools

import jax
import jax.numpy as jnp
from jax import lax
from jax.experimental import pallas as pl
from jax.experimental.pallas import tpu as pltpu
from jax.sharding import PartitionSpec as P

D = 2048
MEMORY_HEADS = 2
KEY_DIM = 256
BLOCK = 128
FF = 1024


epsilon = 1e-06
lowest = -1e30
den_floor = 4.0


def mixer_local(queries, key_vectors, values, input_gate, forget_gate):
    tp_count = lax.axis_size("tp")
    tp_rank = lax.axis_index("tp")
    head_index = tp_rank // (tp_count // MEMORY_HEADS)
    offset = head_index * KEY_DIM
    query_head = lax.dynamic_slice_in_dim(queries, offset, KEY_DIM, 1)
    key_head = lax.dynamic_slice_in_dim(key_vectors, offset, KEY_DIM, 1)
    select = jnp.arange(MEMORY_HEADS, dtype=jnp.int32)[None, :] == head_index
    gates = jnp.stack(
        [
            jnp.sum(jnp.where(select, input_gate, 0.0), axis=1),
            jax.nn.log_sigmoid(jnp.sum(jnp.where(select, forget_gate, 0.0), axis=1)),
        ]
    )
    return query_head, jnp.concatenate([key_head, values], axis=1), gates


def mixer_rows(query_head, both, gates, out_gate):
    ep_count = lax.axis_size("ep")
    ep_rank = lax.axis_index("ep")
    length = query_head.shape[0]
    factor = KEY_DIM ** (-0.5)
    keys_all = both[:, :KEY_DIM]
    values_all = both[:, KEY_DIM:]
    total = ep_count * length
    blocks = total // BLOCK
    mine = length // BLOCK
    input_all = gates[0].reshape(blocks, BLOCK)
    cumulative = jnp.cumsum(gates[1].reshape(blocks, BLOCK), axis=1)
    block_total = cumulative[:, -1]
    index = jnp.arange(blocks, dtype=jnp.int32)
    here = ep_rank * mine + jnp.arange(mine, dtype=jnp.int32)
    between = (index[None, None, :] > index[None, :, None]) & (
        index[None, None, :] < here[:, None, None]
    )
    gap = jnp.sum(jnp.where(between, block_total[None, None, :], 0.0), axis=2)
    ahead = jnp.sum(jnp.where(index[None, :] < here[:, None], block_total[None, :], 0.0), axis=1)
    keep = block_total[:, None] - cumulative + input_all
    own_cumulative = lax.dynamic_slice_in_dim(cumulative, ep_rank * mine, mine, 0)
    same = index[None, :] == here[:, None]
    column = jnp.where(same[:, :, None], input_all - cumulative, keep + gap[:, :, None])
    log_weight = own_cumulative[:, :, None, None] + column[:, None]
    row_at = jnp.arange(BLOCK, dtype=jnp.int32)
    visible = (index[None, :] < here[:, None])[:, None, :, None] | (
        same[:, None, :, None] & (row_at[None, :, None, None] >= row_at[None, None, None, :])
    )
    log_weight = jnp.where(visible, log_weight, -jnp.inf).reshape(length, total)
    carried = (own_cumulative + ahead[:, None]).reshape(length)
    stabilizer = jnp.maximum(carried, jnp.max(log_weight, axis=1))
    within = jnp.exp(log_weight - stabilizer[:, None])
    scores = (
        jnp.einsum("td,sd->ts", query_head, keys_all, preferred_element_type=jnp.float32) * factor
    )
    weights = scores * within
    numerator = jnp.dot(
        weights.astype(jnp.bfloat16), values_all, preferred_element_type=jnp.float32
    )
    denominator = jnp.sum(weights, axis=1)
    hidden = numerator / jnp.maximum(jnp.abs(denominator), den_floor)[:, None]
    gated_rows = (hidden * jax.nn.sigmoid(out_gate.astype(jnp.float32))).astype(jnp.bfloat16)
    return gated_rows


def dense_kernel(
    lines, teams, x_ref, side_ref, kv_ref, sact_ref, g_ref, u_ref, d_ref, sd_ref, mw_ref,
    eo_ref, kvo_ref, so_ref, mwo_ref,
    tok, act, dq, sdq, mwq, sall, kvb, sideb, xout, xin, own, zout, zin, fin,
    z_send, z_recv, x_send, x_recv, c_send, c_recv, a_send, a_recv,
    k_send, k_recv, kx_send, kx_recv, w_send, w_recv, xo_send, xo_recv, zo_send, zo_recv, f_send, f_recv,
):
    me = lax.axis_index("ep")
    j = lax.axis_index("tp")
    z, x = me // 2, me % 2
    tokens = x_ref.shape[0]
    half_rows = tokens // 2
    core = j % 2
    buddy = j + 1 - 2 * core
    quarter = fin.shape[2]
    mine_rows = pl.ds(pl.multiple_of(core * half_rows, half_rows), half_rows)
    other_rows = pl.ds(pl.multiple_of((1 - core) * half_rows, half_rows), half_rows)

    def remote(src, dst, send, recv, ep, tp):
        return pltpu.make_async_remote_copy(
            src_ref=src, dst_ref=dst, send_sem=send, recv_sem=recv,
            device_id={"ep": ep, "tp": tp}, device_id_type=pl.DeviceIdType.MESH,
        )

    barrier = pltpu.get_barrier_semaphore()

    def greet(ep, tp):
        pl.semaphore_signal(
            barrier, inc=1, device_id={"ep": ep, "tp": tp}, device_id_type=pl.DeviceIdType.MESH
        )

    greet(z * 2 + 1 - x, j)
    for k in range(1, lines):
        greet(lax.rem(z + k, lines) * 2 + x, j)
    for k in range(1, teams):
        greet(me, lax.rem(j + k, teams))
    pl.semaphore_wait(barrier, lines + teams - 1)

    def columns(ref, q):
        return ref.at[:, pl.ds(pl.multiple_of(q * quarter, quarter), quarter)]

    def team_copies(k):
        p = lax.rem(j + k, teams)
        pairs = (
            (sact_ref, sall.at[j]),
            (columns(sd_ref, p), sdq.at[j]),
            (columns(mw_ref, p), mwq.at[j]),
            (columns(d_ref, p), dq.at[j]),
        )
        return [
            remote(src, dst, w_send.at[n, k - 1], w_recv.at[n, k - 1], me, p)
            for n, (src, dst) in enumerate(pairs)
        ]

    def z_copy(zb, way):
        to = z + 1 - 2 * way
        ref = tok.at[zb * 2 + x, mine_rows]
        return remote(ref, ref, z_send.at[way, zb], z_recv.at[zb], to * 2 + x, j)

    def x_copy(zb):
        ref = tok.at[zb * 2 + x, mine_rows]
        return remote(ref, ref, x_send.at[zb], x_recv.at[zb], z * 2 + 1 - x, j)

    def x_arrival(zb):
        ref = tok.at[zb * 2 + 1 - x, mine_rows]
        return remote(ref, ref, x_send.at[zb], x_recv.at[zb], z * 2 + 1 - x, j)

    def c_copy(block):
        ref = tok.at[block, mine_rows]
        return remote(ref, ref, c_send.at[block], c_recv.at[block], me, buddy)

    def c_arrival(block):
        ref = tok.at[block, other_rows]
        return remote(ref, ref, c_send.at[block], c_recv.at[block], me, buddy)

    def a_copy(block, k):
        p = lax.rem(j + k, teams)
        return remote(
            act.at[block, j], act.at[block, j],
            a_send.at[block, k - 1], a_recv.at[block, k - 1], me, p,
        )

    def a_arrival(block, k):
        p = lax.rem(j + teams - k, teams)
        return remote(
            act.at[block, p], act.at[block, p],
            a_send.at[block, k - 1], a_recv.at[block, k - 1], me, p,
        )

    extras = (sideb, kvb)

    def k_copy(n, zb, way):
        to = z + 1 - 2 * way
        ref = extras[n].at[zb * 2 + x]
        return remote(ref, ref, k_send.at[n, way, zb], k_recv.at[n, zb], to * 2 + x, j)

    def kx_copy(n, zb):
        ref = extras[n].at[zb * 2 + x]
        return remote(ref, ref, kx_send.at[n, zb], kx_recv.at[n, zb], z * 2 + 1 - x, j)

    def kx_arrival(n, zb):
        ref = extras[n].at[zb * 2 + 1 - x]
        return remote(ref, ref, kx_send.at[n, zb], kx_recv.at[n, zb], z * 2 + 1 - x, j)

    tok[me] = x_ref[...]
    sideb[me] = side_ref[...]
    kvb[me] = kv_ref[...]
    for way in range(2):
        to = z + 1 - 2 * way

        @pl.when((to >= 0) & (to < lines))
        def _():
            remote(
                x_ref.at[mine_rows], tok.at[me, mine_rows],
                z_send.at[way, z], z_recv.at[z], to * 2 + x, j,
            ).start()
            for n, ref in enumerate((side_ref, kv_ref)):
                remote(
                    ref, extras[n].at[me], k_send.at[n, way, z], k_recv.at[n, z], to * 2 + x, j
                ).start()

    remote(
        x_ref.at[mine_rows], tok.at[me, mine_rows], x_send.at[z], x_recv.at[z], z * 2 + 1 - x, j
    ).start()
    for n, ref in enumerate((side_ref, kv_ref)):
        remote(
            ref, extras[n].at[me], kx_send.at[n, z], kx_recv.at[n, z], z * 2 + 1 - x, j
        ).start()
    for k in range(1, teams):
        for copy in team_copies(k):
            copy.start()
    sall[j] = sact_ref[...]
    sdq[j] = columns(sd_ref, j)[...]
    mwq[j] = columns(mw_ref, j)[...]
    dq[j] = columns(d_ref, j)[...]

    def forward(zb, d):
        z_copy(zb, d).wait_recv()
        to = z + 1 - 2 * d

        @pl.when((to >= 0) & (to < lines))
        def _():
            z_copy(zb, d).start()

        x_copy(zb).start()
        c_copy(zb * 2 + x).start()
        for n in range(2):
            k_copy(n, zb, d).wait_recv()

            @pl.when((to >= 0) & (to < lines))
            def _():
                k_copy(n, zb, d).start()

            kx_copy(n, zb).start()

    def activate(block):
        rows = tok[block]
        gate = jnp.dot(rows, g_ref[...], preferred_element_type=jnp.float32)
        up = jnp.dot(rows, u_ref[...], preferred_element_type=jnp.float32)
        act[block, j] = (gate / (1.0 + jnp.exp(-gate)) * up).astype(jnp.bfloat16)
        for k in range(1, teams):
            a_copy(block, k).start()

    def finish(block):
        for k in range(1, teams):
            a_arrival(block, k).wait_recv()
        total = jnp.dot(act[block, 0], dq[0], preferred_element_type=jnp.float32)
        for q in range(1, teams):
            total += jnp.dot(act[block, q], dq[q], preferred_element_type=jnp.float32)
        weight = sideb[block, pl.ds(me, 1), :tokens]
        row = lax.broadcasted_iota(jnp.int32, (tokens, tokens), 0)
        lane = lax.broadcasted_iota(jnp.int32, (tokens, tokens), 1)
        weight = jnp.sum(jnp.where(row == lane, weight, 0.0), axis=1, keepdims=True)
        return (total * weight).astype(jnp.bfloat16)

    def xo_copy(zb):
        return remote(
            xout.at[zb], xin.at[zb], xo_send.at[zb], xo_recv.at[zb], z * 2 + 1 - x, j
        )

    def zo_copy(zb):
        return remote(
            zout.at[zb], zin.at[z], zo_send.at[zb], zo_recv.at[z], zb * 2 + x, j
        )

    def zo_arrival(zb):
        return remote(
            zout.at[zb], zin.at[zb], zo_send.at[zb], zo_recv.at[zb], zb * 2 + x, j
        )

    def valid(s, d, zb):
        return (s >= 0) & (s < lines) & (zb >= 0) & (zb < lines) & ((s > 0) | (d == 0))

    def step(t, carry):
        def stage_one(d, carry):
            s = t
            zb = z + s * (2 * d - 1)

            @pl.when(valid(s, d, zb) & (s > 0))
            def _():
                forward(zb, d)

            return carry

        lax.fori_loop(0, 2, stage_one, 0)

        def stage_two(d, carry):
            s = t - 1
            zb = z + s * (2 * d - 1)

            @pl.when(valid(s, d, zb))
            def _():
                x_arrival(zb).wait_recv()
                c_copy(zb * 2 + 1 - x).start()
                for n in range(2):
                    kx_arrival(n, zb).wait_recv()

                def column(n, carry):
                    block = zb * 2 + lax.rem(x + n, 2)

                    @pl.when(block != me)
                    def _():
                        c_arrival(block).wait_recv()

                    activate(block)
                    return carry

                lax.fori_loop(0, 2, column, 0)

            return carry

        lax.fori_loop(0, 2, stage_two, 0)

        @pl.when(t == 2)
        def _():
            for k in range(1, teams):
                for copy in team_copies(k):
                    copy.wait_recv()

        def stage_three(d, carry):
            s = t - 2
            zb = z + s * (2 * d - 1)

            @pl.when(valid(s, d, zb))
            def _():
                xout[zb] = finish(zb * 2 + 1 - x)
                xo_copy(zb).start()
                own[zb] = finish(zb * 2 + x)

            return carry

        lax.fori_loop(0, 2, stage_three, 0)

        def stage_four(d, carry):
            s = t - 3
            zb = z + s * (2 * d - 1)

            @pl.when(valid(s, d, zb))
            def _():
                xo_copy(zb).wait_recv()

                @pl.when(s > 0)
                def _():
                    zout[zb] = (
                        own[zb].astype(jnp.float32) + xin[zb].astype(jnp.float32)
                    ).astype(jnp.bfloat16)
                    zo_copy(zb).start()

            return carry

        lax.fori_loop(0, 2, stage_four, 0)
        return carry

    lax.fori_loop(1, lines + 3, step, 0)

    def f_copies(k, source, rows):
        p = lax.rem(j + k, teams)
        return remote(
            rows.at[source], rows.at[source],
            f_send.at[k - 1], f_recv.at[k - 1],
            me, p,
        )

    total = own[z].astype(jnp.float32) + xin[z].astype(jnp.float32)
    for q in range(teams):
        total += jnp.dot(sall[q], sdq[q], preferred_element_type=jnp.float32)
    for k in range(1, lines):
        source = lax.rem(z + k, lines)
        zo_arrival(source).wait_recv()
        total += zin[source].astype(jnp.float32)
    fin[j] = total.astype(jnp.bfloat16)
    for k in range(1, teams):
        f_copies(k, j, fin).start()
    kvo_ref[...] = kvb[...]
    so_ref[...] = sideb[...]
    mwo_ref[...] = mwq[...]
    for k in range(1, teams):
        f_copies(k, lax.rem(j + teams - k, teams), fin).wait_recv()
    for q in range(teams):
        eo_ref[:, q * quarter : (q + 1) * quarter] = fin[q]

    for k in range(1, teams):
        f_copies(k, j, fin).wait_send()
        for copy in team_copies(k):
            copy.wait_send()

    def drain(zb, carry):
        for way in range(2):
            to = z + 1 - 2 * way
            passing = (zb <= z) if way == 0 else (zb >= z)

            @pl.when((to >= 0) & (to < lines) & passing)
            def _():
                z_copy(zb, way).wait_send()
                for n in range(2):
                    k_copy(n, zb, way).wait_send()

        x_copy(zb).wait_send()
        for n in range(2):
            kx_copy(n, zb).wait_send()
        xo_copy(zb).wait_send()

        @pl.when(zb != z)
        def _():
            zo_copy(zb).wait_send()

        def column(n, carry):
            block = zb * 2 + n

            @pl.when(block != me)
            def _():
                c_copy(block).wait_send()

            for k in range(1, teams):
                a_copy(block, k).wait_send()
            return carry

        lax.fori_loop(0, 2, column, 0)
        return carry

    lax.fori_loop(0, lines, drain, 0)


def project_kernel(teams, gated_ref, mwq_ref, mo_ref, gall, mfin, g_send, g_recv, f_send, f_recv):
    me = lax.axis_index("ep")
    j = lax.axis_index("tp")
    quarter = mfin.shape[2]

    def copy(ref, source, send, recv, k):
        return pltpu.make_async_remote_copy(
            src_ref=ref, dst_ref=source, send_sem=send.at[k - 1], recv_sem=recv.at[k - 1],
            device_id={"ep": me, "tp": lax.rem(j + k, teams)},
            device_id_type=pl.DeviceIdType.MESH,
        )

    barrier = pltpu.get_barrier_semaphore()
    for k in range(1, teams):
        pl.semaphore_signal(
            barrier, inc=1, device_id={"ep": me, "tp": lax.rem(j + k, teams)},
            device_id_type=pl.DeviceIdType.MESH,
        )
    pl.semaphore_wait(barrier, teams - 1)
    for k in range(1, teams):
        copy(gated_ref, gall.at[j], g_send, g_recv, k).start()
    gall[j] = gated_ref[...]
    for k in range(1, teams):
        source = lax.rem(j + teams - k, teams)
        copy(gated_ref, gall.at[source], g_send, g_recv, k).wait_recv()
    mixed = jnp.zeros(mfin.shape[1:], jnp.float32)
    for q in range(teams):
        mixed += (
            jnp.dot(gall[q], mwq_ref[q], preferred_element_type=jnp.float32)
            .astype(jnp.bfloat16)
            .astype(jnp.float32)
        )
    mfin[j] = mixed.astype(jnp.bfloat16)
    for k in range(1, teams):
        copy(mfin.at[j], mfin.at[j], f_send, f_recv, k).start()
    for k in range(1, teams):
        source = lax.rem(j + teams - k, teams)
        copy(mfin.at[source], mfin.at[source], f_send, f_recv, k).wait_recv()
    for q in range(teams):
        mo_ref[:, q * quarter : (q + 1) * quarter] = mfin[q]
    for k in range(1, teams):
        copy(gated_ref, gall.at[j], g_send, g_recv, k).wait_send()
        copy(mfin.at[j], mfin.at[j], f_send, f_recv, k).wait_send()


def dense_experts(
    query_head,
    both,
    gates,
    out_gate,
    mix_weight,
    expert_input,
    norm_gain,
    route_ids,
    route_weights,
    expert_gate,
    expert_up,
    expert_down,
    shared_gate,
    shared_up,
    shared_down,
):
    ep_count = lax.axis_size("ep")
    teams = lax.axis_size("tp")
    lines = ep_count // 2
    tokens, width = expert_input.shape
    quarter = width // teams
    units = expert_gate.shape[2]
    shared_units = shared_gate.shape[1]
    length, channels = both.shape[0], mix_weight.shape[0]
    rows_wide = expert_input.astype(jnp.float32)
    normed = (
        rows_wide
        * lax.rsqrt(jnp.mean(rows_wide * rows_wide, axis=-1, keepdims=True) + epsilon)
        * norm_gain
    ).astype(jnp.bfloat16)
    named = route_ids[:, :, None] == jnp.arange(ep_count, dtype=jnp.int32)[None, None, :]
    table = jnp.sum(jnp.where(named, route_weights[:, :, None], 0.0), axis=1).T
    lanes = max(tokens, length)
    side = jnp.concatenate(
        [
            jnp.pad(table, ((0, 0), (0, lanes - tokens))),
            jnp.pad(gates, ((0, -(ep_count + 2) % 8), (0, lanes - length))),
        ]
    )
    shared_gate_val = jnp.dot(normed, shared_gate, preferred_element_type=jnp.float32)
    shared_up_val = jnp.dot(normed, shared_up, preferred_element_type=jnp.float32)
    shared_act = (jax.nn.silu(shared_gate_val) * shared_up_val).astype(jnp.bfloat16)
    low, dma = jnp.bfloat16, pltpu.SemaphoreType.DMA
    vmem = pl.BlockSpec(memory_space=pltpu.VMEM)
    expert_out, both_all, side_all, mix_all = pl.pallas_call(
        functools.partial(dense_kernel, lines, teams),
        out_shape=(
            jax.ShapeDtypeStruct((tokens, width), low),
            jax.ShapeDtypeStruct((ep_count, *both.shape), low),
            jax.ShapeDtypeStruct((ep_count, *side.shape), jnp.float32),
            jax.ShapeDtypeStruct((teams, channels, quarter), low),
        ),
        in_specs=[vmem] * 9,
        out_specs=(vmem, vmem, vmem, vmem),
        scratch_shapes=[
            pltpu.VMEM((ep_count, tokens, width), low),
            pltpu.VMEM((ep_count, teams, tokens, units), low),
            pltpu.VMEM((teams, units, quarter), low),
            pltpu.VMEM((teams, shared_units, quarter), low),
            pltpu.VMEM((teams, channels, quarter), low),
            pltpu.VMEM((teams, tokens, shared_units), low),
            pltpu.VMEM((ep_count, *both.shape), low),
            pltpu.VMEM((ep_count, *side.shape), jnp.float32),
            pltpu.VMEM((lines, tokens, quarter), low),
            pltpu.VMEM((lines, tokens, quarter), low),
            pltpu.VMEM((lines, tokens, quarter), low),
            pltpu.VMEM((lines, tokens, quarter), low),
            pltpu.VMEM((lines, tokens, quarter), low),
            pltpu.VMEM((teams, tokens, quarter), low),
            dma((2, lines)), dma((lines,)), dma((lines,)), dma((lines,)),
            dma((ep_count,)), dma((ep_count,)),
            dma((ep_count, teams - 1)), dma((ep_count, teams - 1)),
            dma((2, 2, lines)), dma((2, lines)), dma((2, lines)), dma((2, lines)),
            dma((4, teams - 1)), dma((4, teams - 1)),
            dma((lines,)), dma((lines,)), dma((lines,)), dma((lines,)),
            dma((teams - 1,)), dma((teams - 1,)),
        ],
        compiler_params=pltpu.CompilerParams(
            collective_id=0, has_side_effects=True, vmem_limit_bytes=56 * 1024 * 1024
        ),
    )(
        normed, side, both, shared_act,
        expert_gate[0], expert_up[0], expert_down[0], shared_down, mix_weight,
    )
    gates_all = side_all[:, ep_count : ep_count + 2, :length].transpose(1, 0, 2)
    gated_rows = mixer_rows(
        query_head,
        both_all.reshape(ep_count * length, both.shape[1]),
        gates_all.reshape(2, ep_count * length),
        out_gate,
    )
    mixer_out = pl.pallas_call(
        functools.partial(project_kernel, teams),
        out_shape=jax.ShapeDtypeStruct((length, width), low),
        in_specs=[vmem] * 2,
        out_specs=vmem,
        scratch_shapes=[
            pltpu.VMEM((teams, length, channels), low),
            pltpu.VMEM((teams, length, quarter), low),
            dma((teams - 1,)), dma((teams - 1,)), dma((teams - 1,)), dma((teams - 1,)),
        ],
        compiler_params=pltpu.CompilerParams(collective_id=1, has_side_effects=True),
    )(gated_rows, mix_all)
    return mixer_out, expert_out


def expert_half(
    expert_input,
    norm_gain,
    route_ids,
    route_weights,
    expert_gate,
    expert_up,
    expert_down,
    shared_gate,
    shared_up,
    shared_down,
):
    ep_count = lax.axis_size("ep")
    tp_count = lax.axis_size("tp")
    tp_rank = lax.axis_index("tp")
    tokens = expert_input.shape[0]
    top_count = route_ids.shape[1]
    slice_units = expert_gate.shape[2]
    group_size = FF // slice_units
    per_ep = tp_count // group_size
    team_index = tp_rank // group_size
    expert_count = ep_count * per_ep
    capacity = 2 * tokens * top_count // expert_count
    rows_wide = expert_input.astype(jnp.float32)
    normed = (
        rows_wide
        * lax.rsqrt(jnp.mean(rows_wide * rows_wide, axis=-1, keepdims=True) + epsilon)
        * norm_gain
    ).astype(jnp.bfloat16)
    chosen = route_ids.reshape(-1)
    onehot = (chosen[:, None] == jnp.arange(expert_count, dtype=jnp.int32)[None, :]).astype(
        jnp.int32
    )
    slot_rank = jnp.sum((jnp.cumsum(onehot, axis=0) - onehot) * onehot, axis=1)
    in_team = chosen % per_ep == team_index
    target = jnp.where(in_team, chosen // per_ep * capacity + slot_rank, ep_count * capacity)
    token_of = jnp.arange(chosen.shape[0], dtype=jnp.int32) // top_count
    slot_token = jnp.zeros((ep_count * capacity,), jnp.int32).at[target].set(token_of, mode="drop")
    slot_live = jnp.zeros((ep_count * capacity,), jnp.int32).at[target].set(1, mode="drop")
    outgoing = jnp.where(slot_live[:, None] > 0, normed[slot_token], jnp.zeros((), jnp.bfloat16))
    outgoing = outgoing.reshape(ep_count, capacity, D)
    gate_slice = expert_gate[0]
    up_slice = expert_up[0]
    down_slice = expert_down[0]
    arrived = lax.all_to_all(outgoing, "ep", split_axis=0, concat_axis=0, tiled=True)
    gate_val = jnp.einsum("sid,df->sif", arrived, gate_slice, preferred_element_type=jnp.float32)
    up_val = jnp.einsum("sid,df->sif", arrived, up_slice, preferred_element_type=jnp.float32)
    hidden = (jax.nn.silu(gate_val) * up_val).astype(jnp.bfloat16)
    partial_value = jnp.einsum(
        "sif,fd->sid", hidden, down_slice, preferred_element_type=jnp.float32
    )
    partial_value = partial_value.astype(jnp.bfloat16)
    returned = lax.all_to_all(partial_value, "ep", split_axis=0, concat_axis=0, tiled=True)
    flat_back = returned.reshape(ep_count * capacity, returned.shape[2])
    gather_at = jnp.where(in_team, target, 0).reshape(tokens, top_count)
    weight_at = jnp.where(in_team, route_weights.reshape(-1), 0.0).reshape(tokens, top_count)
    combined = jnp.zeros((tokens, returned.shape[2]), jnp.float32)
    for pick_index in range(top_count):
        combined = (
            combined
            + flat_back[gather_at[:, pick_index]].astype(jnp.float32)
            * weight_at[:, pick_index][:, None]
        )
    shared_gate_val = jnp.dot(normed, shared_gate, preferred_element_type=jnp.float32)
    shared_up_val = jnp.dot(normed, shared_up, preferred_element_type=jnp.float32)
    shared_act = (jax.nn.silu(shared_gate_val) * shared_up_val).astype(jnp.bfloat16)
    return combined + jnp.dot(shared_act, shared_down, preferred_element_type=jnp.float32)


def shards(
    queries,
    key_vectors,
    values,
    out_gate,
    input_gate,
    forget_gate,
    mix_weight,
    expert_input,
    norm_gain,
    route_ids,
    route_weights,
    expert_gate,
    expert_up,
    expert_down,
    shared_gate,
    shared_up,
    shared_down,
):
    ep_count, tp_count = lax.axis_size("ep"), lax.axis_size("tp")
    tokens, slots = expert_input.shape[0], route_ids.shape[1] * 2 * expert_input.shape[0]
    per_ep = tp_count * expert_gate.shape[2] // FF
    even = ep_count % 2 == 0 and tp_count % 2 == 0
    dense = even and per_ep == 1 and slots // (ep_count * per_ep) >= tokens
    query_head, both, gates = mixer_local(
        queries, key_vectors, values, input_gate, forget_gate
    )
    experts = (
        expert_input,
        norm_gain,
        route_ids,
        route_weights,
        expert_gate,
        expert_up,
        expert_down,
        shared_gate,
        shared_up,
        shared_down,
    )
    if dense:
        return dense_experts(query_head, both, gates, out_gate, mix_weight, *experts)
    both = lax.all_gather(both, "ep", axis=0, tiled=True)
    gates = lax.all_gather(gates, "ep", axis=1, tiled=True)
    gated_rows = mixer_rows(query_head, both, gates, out_gate)
    mixer_partial = jnp.dot(gated_rows, mix_weight, preferred_element_type=jnp.float32)
    expert_partial = expert_half(*experts)
    mixer_piece = lax.psum_scatter(
        mixer_partial.astype(jnp.bfloat16), "tp", scatter_dimension=0, tiled=True
    )
    mixer_out = lax.all_gather(mixer_piece, "tp", axis=0, tiled=True)
    expert_piece = lax.psum_scatter(expert_partial, "tp", scatter_dimension=0, tiled=True).astype(
        jnp.bfloat16
    )
    expert_out = lax.all_gather(expert_piece, "tp", axis=0, tiled=True)
    return (mixer_out, expert_out)


def solution(mesh):
    return jax.shard_map(
        shards,
        mesh=mesh,
        in_specs=(
            P("ep", None),
            P("ep", None),
            P("ep", "tp"),
            P("ep", "tp"),
            P("ep", None),
            P("ep", None),
            P("tp", None),
            P("ep", None),
            P(),
            P("ep", None),
            P("ep", None),
            P(("ep", "tp"), None, None),
            P(("ep", "tp"), None, None),
            P(("ep", "tp"), None, None),
            P(None, "tp"),
            P(None, "tp"),
            P("tp", None),
        ),
        out_specs=(P("ep", None), P("ep", None)),
        check_vma=False,
    )
```

```python
import functools

import jax
import jax.numpy as jnp
from jax import lax
from jax.experimental import pallas as pl
from jax.experimental.pallas import tpu as pltpu
from jax.sharding import PartitionSpec as P

D = 2048
MEMORY_HEADS = 2
KEY_DIM = 256
BLOCK = 128
FF = 1024


epsilon = 1e-06
lowest = -1e30
den_floor = 4.0


def mixer_local(queries, key_vectors, values, input_gate, forget_gate):
    tp_count = lax.axis_size("tp")
    tp_rank = lax.axis_index("tp")
    head_index = tp_rank // (tp_count // MEMORY_HEADS)
    offset = head_index * KEY_DIM
    query_head = lax.dynamic_slice_in_dim(queries, offset, KEY_DIM, 1)
    key_head = lax.dynamic_slice_in_dim(key_vectors, offset, KEY_DIM, 1)
    select = jnp.arange(MEMORY_HEADS, dtype=jnp.int32)[None, :] == head_index
    gates = jnp.stack(
        [
            jnp.sum(jnp.where(select, input_gate, 0.0), axis=1),
            jax.nn.log_sigmoid(jnp.sum(jnp.where(select, forget_gate, 0.0), axis=1)),
        ]
    )
    return query_head, jnp.concatenate([key_head, values], axis=1), gates


def mixer_rows(query_head, both, gates, out_gate):
    ep_count = lax.axis_size("ep")
    ep_rank = lax.axis_index("ep")
    length = query_head.shape[0]
    factor = KEY_DIM ** (-0.5)
    keys_all = both[:, :KEY_DIM]
    values_all = both[:, KEY_DIM:]
    total = ep_count * length
    blocks = total // BLOCK
    mine = length // BLOCK
    input_all = gates[0].reshape(blocks, BLOCK)
    cumulative = jnp.cumsum(gates[1].reshape(blocks, BLOCK), axis=1)
    block_total = cumulative[:, -1]
    index = jnp.arange(blocks, dtype=jnp.int32)
    here = ep_rank * mine + jnp.arange(mine, dtype=jnp.int32)
    between = (index[None, None, :] > index[None, :, None]) & (
        index[None, None, :] < here[:, None, None]
    )
    gap = jnp.sum(jnp.where(between, block_total[None, None, :], 0.0), axis=2)
    ahead = jnp.sum(jnp.where(index[None, :] < here[:, None], block_total[None, :], 0.0), axis=1)
    keep = block_total[:, None] - cumulative + input_all
    own_cumulative = lax.dynamic_slice_in_dim(cumulative, ep_rank * mine, mine, 0)
    same = index[None, :] == here[:, None]
    column = jnp.where(same[:, :, None], input_all - cumulative, keep + gap[:, :, None])
    log_weight = own_cumulative[:, :, None, None] + column[:, None]
    row_at = jnp.arange(BLOCK, dtype=jnp.int32)
    visible = (index[None, :] < here[:, None])[:, None, :, None] | (
        same[:, None, :, None] & (row_at[None, :, None, None] >= row_at[None, None, None, :])
    )
    log_weight = jnp.where(visible, log_weight, -jnp.inf).reshape(length, total)
    carried = (own_cumulative + ahead[:, None]).reshape(length)
    stabilizer = jnp.maximum(carried, jnp.max(log_weight, axis=1))
    within = jnp.exp(log_weight - stabilizer[:, None])
    scores = (
        jnp.einsum("td,sd->ts", query_head, keys_all, preferred_element_type=jnp.float32) * factor
    )
    weights = scores * within
    numerator = jnp.dot(
        weights.astype(jnp.bfloat16), values_all, preferred_element_type=jnp.float32
    )
    denominator = jnp.sum(weights, axis=1)
    hidden = numerator / jnp.maximum(jnp.abs(denominator), den_floor)[:, None]
    gated_rows = (hidden * jax.nn.sigmoid(out_gate.astype(jnp.float32))).astype(jnp.bfloat16)
    return gated_rows


def dense_kernel(
    lines, teams, x_ref, side_ref, kv_ref, sact_ref, g_ref, u_ref, d_ref, sd_ref, mw_ref,
    eo_ref, kvo_ref, so_ref, mwo_ref,
    tok, act, dq, sdq, mwq, sall, kvb, sideb, xout, xin, own, zout, zin, fin,
    z_send, z_recv, x_send, x_recv, c_send, c_recv, a_send, a_recv,
    k_send, k_recv, kx_send, kx_recv, w_send, w_recv, xo_send, xo_recv, zo_send, zo_recv, f_send, f_recv,
):
    me = lax.axis_index("ep")
    j = lax.axis_index("tp")
    z, x = me // 2, me % 2
    tokens = x_ref.shape[0]
    half_rows = tokens // 2
    core = j % 2
    buddy = j + 1 - 2 * core
    quarter = fin.shape[2]
    mine_rows = pl.ds(pl.multiple_of(core * half_rows, half_rows), half_rows)
    other_rows = pl.ds(pl.multiple_of((1 - core) * half_rows, half_rows), half_rows)

    def remote(src, dst, send, recv, ep, tp):
        return pltpu.make_async_remote_copy(
            src_ref=src, dst_ref=dst, send_sem=send, recv_sem=recv,
            device_id={"ep": ep, "tp": tp}, device_id_type=pl.DeviceIdType.MESH,
        )

    barrier = pltpu.get_barrier_semaphore()

    def greet(ep, tp):
        pl.semaphore_signal(
            barrier, inc=1, device_id={"ep": ep, "tp": tp}, device_id_type=pl.DeviceIdType.MESH
        )

    greet(z * 2 + 1 - x, j)
    for k in range(1, lines):
        greet(lax.rem(z + k, lines) * 2 + x, j)
    for k in range(1, teams):
        greet(me, lax.rem(j + k, teams))
    pl.semaphore_wait(barrier, lines + teams - 1)

    def columns(ref, q):
        return ref.at[:, pl.ds(pl.multiple_of(q * quarter, quarter), quarter)]

    def team_copies(k):
        p = lax.rem(j + k, teams)
        pairs = (
            (sact_ref, sall.at[j]),
            (columns(sd_ref, p), sdq.at[j]),
            (columns(mw_ref, p), mwq.at[j]),
            (columns(d_ref, p), dq.at[j]),
        )
        return [
            remote(src, dst, w_send.at[n, k - 1], w_recv.at[n, k - 1], me, p)
            for n, (src, dst) in enumerate(pairs)
        ]

    def z_copy(zb, way):
        to = z + 1 - 2 * way
        ref = tok.at[zb * 2 + x, mine_rows]
        return remote(ref, ref, z_send.at[way, zb], z_recv.at[zb], to * 2 + x, j)

    def x_copy(zb):
        ref = tok.at[zb * 2 + x, mine_rows]
        return remote(ref, ref, x_send.at[zb], x_recv.at[zb], z * 2 + 1 - x, j)

    def x_arrival(zb):
        ref = tok.at[zb * 2 + 1 - x, mine_rows]
        return remote(ref, ref, x_send.at[zb], x_recv.at[zb], z * 2 + 1 - x, j)

    def c_copy(block):
        ref = tok.at[block, mine_rows]
        return remote(ref, ref, c_send.at[block], c_recv.at[block], me, buddy)

    def c_arrival(block):
        ref = tok.at[block, other_rows]
        return remote(ref, ref, c_send.at[block], c_recv.at[block], me, buddy)

    def a_copy(block, k):
        p = lax.rem(j + k, teams)
        return remote(
            act.at[block, j], act.at[block, j],
            a_send.at[block, k - 1], a_recv.at[block, k - 1], me, p,
        )

    extras = (sideb, kvb)

    def k_copy(n, zb, way):
        to = z + 1 - 2 * way
        ref = extras[n].at[zb * 2 + x]
        return remote(ref, ref, k_send.at[n, way, zb], k_recv.at[n, zb], to * 2 + x, j)

    def kx_copy(n, zb):
        ref = extras[n].at[zb * 2 + x]
        return remote(ref, ref, kx_send.at[n, zb], kx_recv.at[n, zb], z * 2 + 1 - x, j)

    def kx_arrival(n, zb):
        ref = extras[n].at[zb * 2 + 1 - x]
        return remote(ref, ref, kx_send.at[n, zb], kx_recv.at[n, zb], z * 2 + 1 - x, j)

    tok[me] = x_ref[...]
    sideb[me] = side_ref[...]
    kvb[me] = kv_ref[...]
    for way in range(2):
        to = z + 1 - 2 * way

        @pl.when((to >= 0) & (to < lines))
        def _():
            remote(
                x_ref.at[mine_rows], tok.at[me, mine_rows],
                z_send.at[way, z], z_recv.at[z], to * 2 + x, j,
            ).start()
            for n, ref in enumerate((side_ref, kv_ref)):
                remote(
                    ref, extras[n].at[me], k_send.at[n, way, z], k_recv.at[n, z], to * 2 + x, j
                ).start()

    remote(
        x_ref.at[mine_rows], tok.at[me, mine_rows], x_send.at[z], x_recv.at[z], z * 2 + 1 - x, j
    ).start()
    for n, ref in enumerate((side_ref, kv_ref)):
        remote(
            ref, extras[n].at[me], kx_send.at[n, z], kx_recv.at[n, z], z * 2 + 1 - x, j
        ).start()
    for k in range(1, teams):
        for copy in team_copies(k):
            copy.start()
    sall[j] = sact_ref[...]
    sdq[j] = columns(sd_ref, j)[...]
    mwq[j] = columns(mw_ref, j)[...]
    dq[j] = columns(d_ref, j)[...]

    def forward(zb, d):
        z_copy(zb, d).wait_recv()
        to = z + 1 - 2 * d

        @pl.when((to >= 0) & (to < lines))
        def _():
            z_copy(zb, d).start()

        x_copy(zb).start()
        c_copy(zb * 2 + x).start()
        for n in range(2):
            k_copy(n, zb, d).wait_recv()

            @pl.when((to >= 0) & (to < lines))
            def _():
                k_copy(n, zb, d).start()

            kx_copy(n, zb).start()

    def activate(block):
        rows = tok[block]
        gate = jnp.dot(rows, g_ref[...], preferred_element_type=jnp.float32)
        up = jnp.dot(rows, u_ref[...], preferred_element_type=jnp.float32)
        act[block, j] = (gate / (1.0 + jnp.exp(-gate)) * up).astype(jnp.bfloat16)
        for e in range(1, teams // 2):
            a_move(block, j, e - 1, lax.rem(j + 2 * e, teams)).start()
        a_move(block, j, teams // 2 - 1, buddy).start()

    def a_move(block, source, slot, to):
        ref = act.at[block, source]
        return remote(ref, ref, a_send.at[block, slot], a_recv.at[block, slot], me, to)

    def finish(block):
        for e in range(1, teams // 2):
            source = lax.rem(j + teams - 2 * e, teams)
            a_move(block, source, e - 1, source).wait_recv()
            a_move(block, source, teams // 2 - 1 + e, buddy).start()
        for e in range(teams // 2):
            source = lax.rem(buddy + teams - 2 * e, teams)
            a_move(block, source, teams // 2 - 1 + e, buddy).wait_recv()
        total = jnp.dot(act[block, 0], dq[0], preferred_element_type=jnp.float32)
        for q in range(1, teams):
            total += jnp.dot(act[block, q], dq[q], preferred_element_type=jnp.float32)
        weight = sideb[block, pl.ds(me, 1), :tokens]
        row = lax.broadcasted_iota(jnp.int32, (tokens, tokens), 0)
        lane = lax.broadcasted_iota(jnp.int32, (tokens, tokens), 1)
        weight = jnp.sum(jnp.where(row == lane, weight, 0.0), axis=1, keepdims=True)
        return (total * weight).astype(jnp.bfloat16)

    def xo_copy(zb):
        return remote(
            xout.at[zb], xin.at[zb], xo_send.at[zb], xo_recv.at[zb], z * 2 + 1 - x, j
        )

    def zo_copy(zb):
        return remote(
            zout.at[zb], zin.at[z], zo_send.at[zb], zo_recv.at[z], zb * 2 + x, j
        )

    def zo_arrival(zb):
        return remote(
            zout.at[zb], zin.at[zb], zo_send.at[zb], zo_recv.at[zb], zb * 2 + x, j
        )

    def valid(s, d, zb):
        return (s >= 0) & (s < lines) & (zb >= 0) & (zb < lines) & ((s > 0) | (d == 0))

    def step(t, carry):
        def stage_one(d, carry):
            s = t
            zb = z + s * (2 * d - 1)

            @pl.when(valid(s, d, zb) & (s > 0))
            def _():
                forward(zb, d)

            return carry

        lax.fori_loop(0, 2, stage_one, 0)

        def stage_two(d, carry):
            s = t - 1
            zb = z + s * (2 * d - 1)

            @pl.when(valid(s, d, zb))
            def _():
                x_arrival(zb).wait_recv()
                c_copy(zb * 2 + 1 - x).start()
                for n in range(2):
                    kx_arrival(n, zb).wait_recv()

                def column(n, carry):
                    block = zb * 2 + lax.rem(x + n, 2)

                    @pl.when(block != me)
                    def _():
                        c_arrival(block).wait_recv()

                    activate(block)
                    return carry

                lax.fori_loop(0, 2, column, 0)

            return carry

        lax.fori_loop(0, 2, stage_two, 0)

        @pl.when(t == 2)
        def _():
            for k in range(1, teams):
                for copy in team_copies(k):
                    copy.wait_recv()

        def stage_three(d, carry):
            s = t - 2
            zb = z + s * (2 * d - 1)

            @pl.when(valid(s, d, zb))
            def _():
                xout[zb] = finish(zb * 2 + 1 - x)
                xo_copy(zb).start()
                own[zb] = finish(zb * 2 + x)

            return carry

        lax.fori_loop(0, 2, stage_three, 0)

        def stage_four(d, carry):
            s = t - 3
            zb = z + s * (2 * d - 1)

            @pl.when(valid(s, d, zb))
            def _():
                xo_copy(zb).wait_recv()

                @pl.when(s > 0)
                def _():
                    zout[zb] = (
                        own[zb].astype(jnp.float32) + xin[zb].astype(jnp.float32)
                    ).astype(jnp.bfloat16)
                    zo_copy(zb).start()

            return carry

        lax.fori_loop(0, 2, stage_four, 0)
        return carry

    lax.fori_loop(1, lines + 3, step, 0)

    def f_copies(k, source, rows):
        p = lax.rem(j + k, teams)
        return remote(
            rows.at[source], rows.at[source],
            f_send.at[k - 1], f_recv.at[k - 1],
            me, p,
        )

    total = own[z].astype(jnp.float32) + xin[z].astype(jnp.float32)
    for q in range(teams):
        total += jnp.dot(sall[q], sdq[q], preferred_element_type=jnp.float32)
    for k in range(1, lines):
        source = lax.rem(z + k, lines)
        zo_arrival(source).wait_recv()
        total += zin[source].astype(jnp.float32)
    fin[j] = total.astype(jnp.bfloat16)
    for k in range(1, teams):
        f_copies(k, j, fin).start()
    kvo_ref[...] = kvb[...]
    so_ref[...] = sideb[...]
    mwo_ref[...] = mwq[...]
    for k in range(1, teams):
        f_copies(k, lax.rem(j + teams - k, teams), fin).wait_recv()
    for q in range(teams):
        eo_ref[:, q * quarter : (q + 1) * quarter] = fin[q]

    for k in range(1, teams):
        f_copies(k, j, fin).wait_send()
        for copy in team_copies(k):
            copy.wait_send()

    def drain(zb, carry):
        for way in range(2):
            to = z + 1 - 2 * way
            passing = (zb <= z) if way == 0 else (zb >= z)

            @pl.when((to >= 0) & (to < lines) & passing)
            def _():
                z_copy(zb, way).wait_send()
                for n in range(2):
                    k_copy(n, zb, way).wait_send()

        x_copy(zb).wait_send()
        for n in range(2):
            kx_copy(n, zb).wait_send()
        xo_copy(zb).wait_send()

        @pl.when(zb != z)
        def _():
            zo_copy(zb).wait_send()

        def column(n, carry):
            block = zb * 2 + n

            @pl.when(block != me)
            def _():
                c_copy(block).wait_send()

            for k in range(1, teams):
                a_copy(block, k).wait_send()
            return carry

        lax.fori_loop(0, 2, column, 0)
        return carry

    lax.fori_loop(0, lines, drain, 0)


def project_kernel(teams, gated_ref, mwq_ref, mo_ref, gall, mfin, g_send, g_recv, f_send, f_recv):
    me = lax.axis_index("ep")
    j = lax.axis_index("tp")
    quarter = mfin.shape[2]

    def copy(ref, source, send, recv, k):
        return pltpu.make_async_remote_copy(
            src_ref=ref, dst_ref=source, send_sem=send.at[k - 1], recv_sem=recv.at[k - 1],
            device_id={"ep": me, "tp": lax.rem(j + k, teams)},
            device_id_type=pl.DeviceIdType.MESH,
        )

    barrier = pltpu.get_barrier_semaphore()
    for k in range(1, teams):
        pl.semaphore_signal(
            barrier, inc=1, device_id={"ep": me, "tp": lax.rem(j + k, teams)},
            device_id_type=pl.DeviceIdType.MESH,
        )
    pl.semaphore_wait(barrier, teams - 1)
    for k in range(1, teams):
        copy(gated_ref, gall.at[j], g_send, g_recv, k).start()
    gall[j] = gated_ref[...]
    for k in range(1, teams):
        source = lax.rem(j + teams - k, teams)
        copy(gated_ref, gall.at[source], g_send, g_recv, k).wait_recv()
    mixed = jnp.zeros(mfin.shape[1:], jnp.float32)
    for q in range(teams):
        mixed += (
            jnp.dot(gall[q], mwq_ref[q], preferred_element_type=jnp.float32)
            .astype(jnp.bfloat16)
            .astype(jnp.float32)
        )
    mfin[j] = mixed.astype(jnp.bfloat16)
    for k in range(1, teams):
        copy(mfin.at[j], mfin.at[j], f_send, f_recv, k).start()
    for k in range(1, teams):
        source = lax.rem(j + teams - k, teams)
        copy(mfin.at[source], mfin.at[source], f_send, f_recv, k).wait_recv()
    for q in range(teams):
        mo_ref[:, q * quarter : (q + 1) * quarter] = mfin[q]
    for k in range(1, teams):
        copy(gated_ref, gall.at[j], g_send, g_recv, k).wait_send()
        copy(mfin.at[j], mfin.at[j], f_send, f_recv, k).wait_send()


def dense_experts(
    query_head,
    both,
    gates,
    out_gate,
    mix_weight,
    expert_input,
    norm_gain,
    route_ids,
    route_weights,
    expert_gate,
    expert_up,
    expert_down,
    shared_gate,
    shared_up,
    shared_down,
):
    ep_count = lax.axis_size("ep")
    teams = lax.axis_size("tp")
    lines = ep_count // 2
    tokens, width = expert_input.shape
    quarter = width // teams
    units = expert_gate.shape[2]
    shared_units = shared_gate.shape[1]
    length, channels = both.shape[0], mix_weight.shape[0]
    rows_wide = expert_input.astype(jnp.float32)
    normed = (
        rows_wide
        * lax.rsqrt(jnp.mean(rows_wide * rows_wide, axis=-1, keepdims=True) + epsilon)
        * norm_gain
    ).astype(jnp.bfloat16)
    named = route_ids[:, :, None] == jnp.arange(ep_count, dtype=jnp.int32)[None, None, :]
    table = jnp.sum(jnp.where(named, route_weights[:, :, None], 0.0), axis=1).T
    lanes = max(tokens, length)
    side = jnp.concatenate(
        [
            jnp.pad(table, ((0, 0), (0, lanes - tokens))),
            jnp.pad(gates, ((0, -(ep_count + 2) % 8), (0, lanes - length))),
        ]
    )
    shared_gate_val = jnp.dot(normed, shared_gate, preferred_element_type=jnp.float32)
    shared_up_val = jnp.dot(normed, shared_up, preferred_element_type=jnp.float32)
    shared_act = (jax.nn.silu(shared_gate_val) * shared_up_val).astype(jnp.bfloat16)
    low, dma = jnp.bfloat16, pltpu.SemaphoreType.DMA
    vmem = pl.BlockSpec(memory_space=pltpu.VMEM)
    expert_out, both_all, side_all, mix_all = pl.pallas_call(
        functools.partial(dense_kernel, lines, teams),
        out_shape=(
            jax.ShapeDtypeStruct((tokens, width), low),
            jax.ShapeDtypeStruct((ep_count, *both.shape), low),
            jax.ShapeDtypeStruct((ep_count, *side.shape), jnp.float32),
            jax.ShapeDtypeStruct((teams, channels, quarter), low),
        ),
        in_specs=[vmem] * 9,
        out_specs=(vmem, vmem, vmem, vmem),
        scratch_shapes=[
            pltpu.VMEM((ep_count, tokens, width), low),
            pltpu.VMEM((ep_count, teams, tokens, units), low),
            pltpu.VMEM((teams, units, quarter), low),
            pltpu.VMEM((teams, shared_units, quarter), low),
            pltpu.VMEM((teams, channels, quarter), low),
            pltpu.VMEM((teams, tokens, shared_units), low),
            pltpu.VMEM((ep_count, *both.shape), low),
            pltpu.VMEM((ep_count, *side.shape), jnp.float32),
            pltpu.VMEM((lines, tokens, quarter), low),
            pltpu.VMEM((lines, tokens, quarter), low),
            pltpu.VMEM((lines, tokens, quarter), low),
            pltpu.VMEM((lines, tokens, quarter), low),
            pltpu.VMEM((lines, tokens, quarter), low),
            pltpu.VMEM((teams, tokens, quarter), low),
            dma((2, lines)), dma((lines,)), dma((lines,)), dma((lines,)),
            dma((ep_count,)), dma((ep_count,)),
            dma((ep_count, teams - 1)), dma((ep_count, teams - 1)),
            dma((2, 2, lines)), dma((2, lines)), dma((2, lines)), dma((2, lines)),
            dma((4, teams - 1)), dma((4, teams - 1)),
            dma((lines,)), dma((lines,)), dma((lines,)), dma((lines,)),
            dma((teams - 1,)), dma((teams - 1,)),
        ],
        compiler_params=pltpu.CompilerParams(
            collective_id=0, has_side_effects=True, vmem_limit_bytes=56 * 1024 * 1024
        ),
    )(
        normed, side, both, shared_act,
        expert_gate[0], expert_up[0], expert_down[0], shared_down, mix_weight,
    )
    gates_all = side_all[:, ep_count : ep_count + 2, :length].transpose(1, 0, 2)
    gated_rows = mixer_rows(
        query_head,
        both_all.reshape(ep_count * length, both.shape[1]),
        gates_all.reshape(2, ep_count * length),
        out_gate,
    )
    mixer_out = pl.pallas_call(
        functools.partial(project_kernel, teams),
        out_shape=jax.ShapeDtypeStruct((length, width), low),
        in_specs=[vmem] * 2,
        out_specs=vmem,
        scratch_shapes=[
            pltpu.VMEM((teams, length, channels), low),
            pltpu.VMEM((teams, length, quarter), low),
            dma((teams - 1,)), dma((teams - 1,)), dma((teams - 1,)), dma((teams - 1,)),
        ],
        compiler_params=pltpu.CompilerParams(collective_id=1, has_side_effects=True),
    )(gated_rows, mix_all)
    return mixer_out, expert_out


def expert_half(
    expert_input,
    norm_gain,
    route_ids,
    route_weights,
    expert_gate,
    expert_up,
    expert_down,
    shared_gate,
    shared_up,
    shared_down,
):
    ep_count = lax.axis_size("ep")
    tp_count = lax.axis_size("tp")
    tp_rank = lax.axis_index("tp")
    tokens = expert_input.shape[0]
    top_count = route_ids.shape[1]
    slice_units = expert_gate.shape[2]
    group_size = FF // slice_units
    per_ep = tp_count // group_size
    team_index = tp_rank // group_size
    expert_count = ep_count * per_ep
    capacity = 2 * tokens * top_count // expert_count
    rows_wide = expert_input.astype(jnp.float32)
    normed = (
        rows_wide
        * lax.rsqrt(jnp.mean(rows_wide * rows_wide, axis=-1, keepdims=True) + epsilon)
        * norm_gain
    ).astype(jnp.bfloat16)
    chosen = route_ids.reshape(-1)
    onehot = (chosen[:, None] == jnp.arange(expert_count, dtype=jnp.int32)[None, :]).astype(
        jnp.int32
    )
    slot_rank = jnp.sum((jnp.cumsum(onehot, axis=0) - onehot) * onehot, axis=1)
    in_team = chosen % per_ep == team_index
    target = jnp.where(in_team, chosen // per_ep * capacity + slot_rank, ep_count * capacity)
    token_of = jnp.arange(chosen.shape[0], dtype=jnp.int32) // top_count
    slot_token = jnp.zeros((ep_count * capacity,), jnp.int32).at[target].set(token_of, mode="drop")
    slot_live = jnp.zeros((ep_count * capacity,), jnp.int32).at[target].set(1, mode="drop")
    outgoing = jnp.where(slot_live[:, None] > 0, normed[slot_token], jnp.zeros((), jnp.bfloat16))
    outgoing = outgoing.reshape(ep_count, capacity, D)
    gate_slice = expert_gate[0]
    up_slice = expert_up[0]
    down_slice = expert_down[0]
    arrived = lax.all_to_all(outgoing, "ep", split_axis=0, concat_axis=0, tiled=True)
    gate_val = jnp.einsum("sid,df->sif", arrived, gate_slice, preferred_element_type=jnp.float32)
    up_val = jnp.einsum("sid,df->sif", arrived, up_slice, preferred_element_type=jnp.float32)
    hidden = (jax.nn.silu(gate_val) * up_val).astype(jnp.bfloat16)
    partial_value = jnp.einsum(
        "sif,fd->sid", hidden, down_slice, preferred_element_type=jnp.float32
    )
    partial_value = partial_value.astype(jnp.bfloat16)
    returned = lax.all_to_all(partial_value, "ep", split_axis=0, concat_axis=0, tiled=True)
    flat_back = returned.reshape(ep_count * capacity, returned.shape[2])
    gather_at = jnp.where(in_team, target, 0).reshape(tokens, top_count)
    weight_at = jnp.where(in_team, route_weights.reshape(-1), 0.0).reshape(tokens, top_count)
    combined = jnp.zeros((tokens, returned.shape[2]), jnp.float32)
    for pick_index in range(top_count):
        combined = (
            combined
            + flat_back[gather_at[:, pick_index]].astype(jnp.float32)
            * weight_at[:, pick_index][:, None]
        )
    shared_gate_val = jnp.dot(normed, shared_gate, preferred_element_type=jnp.float32)
    shared_up_val = jnp.dot(normed, shared_up, preferred_element_type=jnp.float32)
    shared_act = (jax.nn.silu(shared_gate_val) * shared_up_val).astype(jnp.bfloat16)
    return combined + jnp.dot(shared_act, shared_down, preferred_element_type=jnp.float32)


def shards(
    queries,
    key_vectors,
    values,
    out_gate,
    input_gate,
    forget_gate,
    mix_weight,
    expert_input,
    norm_gain,
    route_ids,
    route_weights,
    expert_gate,
    expert_up,
    expert_down,
    shared_gate,
    shared_up,
    shared_down,
):
    ep_count, tp_count = lax.axis_size("ep"), lax.axis_size("tp")
    tokens, slots = expert_input.shape[0], route_ids.shape[1] * 2 * expert_input.shape[0]
    per_ep = tp_count * expert_gate.shape[2] // FF
    even = ep_count % 2 == 0 and tp_count % 2 == 0
    dense = even and per_ep == 1 and slots // (ep_count * per_ep) >= tokens
    query_head, both, gates = mixer_local(
        queries, key_vectors, values, input_gate, forget_gate
    )
    experts = (
        expert_input,
        norm_gain,
        route_ids,
        route_weights,
        expert_gate,
        expert_up,
        expert_down,
        shared_gate,
        shared_up,
        shared_down,
    )
    if dense:
        return dense_experts(query_head, both, gates, out_gate, mix_weight, *experts)
    both = lax.all_gather(both, "ep", axis=0, tiled=True)
    gates = lax.all_gather(gates, "ep", axis=1, tiled=True)
    gated_rows = mixer_rows(query_head, both, gates, out_gate)
    mixer_partial = jnp.dot(gated_rows, mix_weight, preferred_element_type=jnp.float32)
    expert_partial = expert_half(*experts)
    mixer_piece = lax.psum_scatter(
        mixer_partial.astype(jnp.bfloat16), "tp", scatter_dimension=0, tiled=True
    )
    mixer_out = lax.all_gather(mixer_piece, "tp", axis=0, tiled=True)
    expert_piece = lax.psum_scatter(expert_partial, "tp", scatter_dimension=0, tiled=True).astype(
        jnp.bfloat16
    )
    expert_out = lax.all_gather(expert_piece, "tp", axis=0, tiled=True)
    return (mixer_out, expert_out)


def solution(mesh):
    return jax.shard_map(
        shards,
        mesh=mesh,
        in_specs=(
            P("ep", None),
            P("ep", None),
            P("ep", "tp"),
            P("ep", "tp"),
            P("ep", None),
            P("ep", None),
            P("tp", None),
            P("ep", None),
            P(),
            P("ep", None),
            P("ep", None),
            P(("ep", "tp"), None, None),
            P(("ep", "tp"), None, None),
            P(("ep", "tp"), None, None),
            P(None, "tp"),
            P(None, "tp"),
            P("tp", None),
        ),
        out_specs=(P("ep", None), P("ep", None)),
        check_vma=False,
    )
```
